32 devices in a mesh: dp: 4 (over y, x), kv: 4 (over z), tp: 2 (over core).
Axes of the slice: x: 2, y: 2, z: 4, core: 2. Of those that a mesh axis runs over, the one named last changes fastest.
Arguments:
- hidden: bfloat16 [2048, 16], P(('kv', 'tp'), 'dp'), parts along dimension 1, may hold values from -20 to 20
- mixer_gain: float32 [2048], replicated, may hold values from 0.1 to 1.9
- gate_proj: bfloat16 [2048, 64, 64], P(None, 'kv', 'tp'), may hold values from -0.125 to 0.125
- inner_proj: bfloat16 [2048, 64, 64], P(None, 'kv', 'tp'), may hold values from -0.125 to 0.125
- input_proj: bfloat16 [2048, 1024], P(None, 'kv'), may hold values from -0.125 to 0.125
- output_proj: bfloat16 [2048, 1024], P(None, 'kv'), may hold values from -0.125 to 0.125
- step_proj: bfloat16 [2048, 64], replicated, may hold values from -0.125 to 0.125
- step_bias: float32 [64], replicated, may hold values from -3 to -0.5
- decay_log: float32 [64], replicated, may hold values from -3 to 1
- skip_gain: float32 [64], replicated, may hold values from 0.3 to 1.5
- taps_inner: float32 [4, 64, 64], P(None, None, 'tp'), may hold values from -3 to 3
- taps_input: float32 [4, 1024], replicated, may hold values from -3 to 3
- taps_output: float32 [4, 1024], replicated, may hold values from -3 to 3
- recent_inner: bfloat16 [16, 3, 64, 64], P(('dp', 'kv'), None, None, 'tp'), parts along dimension 0, may hold values from -6 to 6
- recent_input: bfloat16 [16, 3, 1024], P(('dp', 'kv')), parts along dimension 0, may hold values from -6 to 6
- recent_output: bfloat16 [16, 3, 1024], P(('dp', 'kv')), parts along dimension 0, may hold values from -6 to 6
- states: float32 [16, 64, 64, 128], P(('dp', 'kv'), None, 'tp'), parts along dimension 0, may hold values from -4 to 4
- block_inner: bfloat16 [16, 128, 64, 64], P(('dp', 'kv'), None, None, 'tp'), parts along dimension 0, may hold values from -6 to 6
- block_input: bfloat16 [16, 128, 1024], P(('dp', 'kv')), parts along dimension 0, may hold values from -4 to 4
- block_decay: float32 [16, 128, 64], P(('dp', 'kv')), parts along dimension 0
- lengths: int32 [16], P(('dp', 'kv')), parts along dimension 0, may hold values from 1 to 128, 170 in all
- norm_gain: float32 [64, 64], P(None, 'tp'), may hold values from 0.1 to 1.9
- mixer_out: bfloat16 [64, 64, 2048], P('kv', 'tp'), may hold values from -0.125 to 0.125
- channel_gain: float32 [2048], replicated, may hold values from 0.1 to 1.9
- expand_gate: bfloat16 [2048, 5632], P(None, ('kv', 'tp')), may hold values from -0.125 to 0.125
- expand_value: bfloat16 [2048, 5632], P(None, ('kv', 'tp')), may hold values from -0.125 to 0.125
- reduce_proj: bfloat16 [5632, 2048], P(('kv', 'tp')), may hold values from -0.109375 to 0.109375
Outputs:
- layer_out: bfloat16 [2048, 16], P(('kv', 'tp'), 'dp'), parts along dimension 1
The draws below stay inside these ranges and needn't reach their ends.
There are 4 independent parts, one for each index of `dp`. The reference program is written for one: setup_inputs(seed, part) draws one part's arguments, and reference() takes and returns one part's arrays. A program takes and returns all parts, laid end to end along the dimension named above; an argument that names none is the same for every part. Nothing has to cross between parts.
All inputs are finite; a program needn't handle non-finite values. No bound on the sum of `lengths` on one device may be relied on, other than what follows from the above.
Results may differ from the reference program's by a relative error of at most 0.01.
Values may be sent and summed in bfloat16 or wider, within the bound.
No kernel may reach another device: no remote copies, remote signals or barrier semaphores. Data moves between devices by JAX's collectives and lax.ppermute only.
A program may use at most 64 MiB of HBM per device.

```python
import math
import jax
import jax.numpy as jnp
import numpy as np
from jax import lax

D = 2048
MIXER_HEADS = 64
HEAD_DIM = 64
GROUPS = 8
STATE = 128
FF = 5632
TAPS = 4
OPEN_BLOCK_SPAN = 128
GROUP_SEQUENCES = 4


def draw_hidden(key, part):
    rows = jnp.arange(D, dtype=jnp.float32)[:, None] / D
    rising = 1.0 + 2.0 * rows
    base = jax.random.truncated_normal(key, -4.0, 4.0, (D, GROUP_SEQUENCES), jnp.float32)
    return (base * rising).astype(jnp.bfloat16)


def draw_block_decay(key, part):
    key_rate, key_seq, key_jitter, position_key, extent_key = jax.random.split(jax.random.fold_in(key, 17), 5)
    low, high = (math.log(0.2 / OPEN_BLOCK_SPAN), math.log(0.08))
    arrival_rate = jnp.exp(jax.random.uniform(key_rate, (1, 1, MIXER_HEADS), jnp.float32, low, high))
    sequence_share = jnp.exp(jax.random.uniform(key_seq, (GROUP_SEQUENCES, 1, 1), jnp.float32, math.log(0.5), math.log(2.0)))
    random_shift = jnp.exp(jax.random.uniform(key_jitter, (GROUP_SEQUENCES, OPEN_BLOCK_SPAN, MIXER_HEADS), jnp.float32, -0.35, 0.35))
    surge_position = (jax.random.randint(position_key, (GROUP_SEQUENCES, OPEN_BLOCK_SPAN, 1), 0, OPEN_BLOCK_SPAN) < 3).astype(jnp.float32)
    surge_extent = jax.random.uniform(extent_key, (GROUP_SEQUENCES, OPEN_BLOCK_SPAN, MIXER_HEADS), jnp.float32, 0.22, 0.69)
    return -(arrival_rate * sequence_share * random_shift) - surge_position * surge_extent


def raised(result, own_key, source, target, shards_of, factor):
    def block_of(position):
        return (jnp.arange(result.shape[position]) // (result.shape[position] // shards_of)).reshape((-1,) + (1,) * (result.ndim - 1 - position))

    one_side = jax.random.permutation(own_key, shards_of)[block_of(target)]
    other_side = (block_of(target) + shards_of // 2) % shards_of
    return jnp.where((block_of(source) == one_side) | (block_of(source) == other_side), factor * result, result)


def shard_levels(key, extent, shards, least, high):
    loudness = 1.0
    for position, shards_of in shards:
        draws = jax.random.uniform(jax.random.fold_in(jax.random.fold_in(key, 6), position), (shards_of,), jnp.float32, least / len(shards), high / len(shards))
        loudness = loudness * jnp.repeat(jnp.exp(draws), extent[position] // shards_of).reshape((-1,) + (1,) * (len(extent) - 1 - position))
    return loudness


def profile(count, total, reach, skew):
    portions = [(1 << 20) // math.isqrt(standing ** skew) + 1 for standing in range(2, count + 1)]
    rest, counts = total - reach - (count - 1), [1] * (count - 1)
    while rest > 0:
        movable = [i for i in range(count - 1) if counts[i] < reach]
        whole, budget = sum([portions[i] for i in movable]), rest
        for i in movable:
            extra = min(reach - counts[i], max(1, budget * portions[i] // whole), rest)
            counts[i] = counts[i] + extra
            rest = rest - extra
    return np.array([reach] + counts)


def uneven_parts(own_key, number_of, total, most, lean):
    if number_of == 2:
        one = jax.random.randint(own_key, (), max(1, total - most), min(most, total - 1) + 1)
        return jnp.stack([one, total - one])
    sizes = jnp.asarray(profile(number_of, total, most, lean), jnp.int32)
    pairs = (number_of - 1) // 2
    source_of, sink = sizes[1:1 + 2 * pairs:2], sizes[2:2 + 2 * pairs:2]
    room = jnp.minimum(source_of - 1, most - sink)
    moved = jax.random.randint(jax.random.fold_in(own_key, 1), (pairs,), 0, 1 << 20) % (room + 1)
    sizes = sizes.at[1:1 + 2 * pairs:2].set(source_of - moved).at[2:2 + 2 * pairs:2].set(sink + moved)
    return sizes[jax.random.permutation(jax.random.fold_in(own_key, 2), number_of)]


def centred(rng, shape, deviation, bound, cuts=(), kind=jnp.bfloat16):
    entries = deviation * jax.random.normal(rng, shape, jnp.float32)
    if cuts:
        entries = entries * shard_levels(rng, shape, cuts, -0.22, 0.18)
    return jnp.clip(entries, -bound, bound).astype(kind)


def bell_draw_with(stream_key, dims, width, reach, cuts, heavy, kind=jnp.bfloat16):
    array = width * jax.random.normal(stream_key, dims, jnp.float32)
    if cuts:
        array = array * shard_levels(stream_key, dims, cuts, -0.22, 0.18)
    return jnp.clip(raised(array, jax.random.fold_in(stream_key, 3), *heavy), -reach, reach).astype(kind)


def setup_inputs(seed: int = 0, part: int = 0) -> dict:
    seeds = jax.random.split(jax.random.key(seed), 28)
    part_keys = jax.random.split(jax.random.fold_in(seeds[27], part), 28)
    hidden = draw_hidden(jax.random.fold_in(jax.random.fold_in(seeds[27], part), 71), part)
    mixer_gain = jnp.clip(1.0 + 0.18 * jax.random.normal(seeds[1], (D,), jnp.float32), 0.1, 1.9)
    gate_proj = centred(seeds[2], (D, MIXER_HEADS, HEAD_DIM), D ** -0.5, 0.125, ((1, 4), (2, 2)))
    inner_proj = centred(seeds[3], (D, MIXER_HEADS, HEAD_DIM), D ** -0.5, 0.125, ((1, 4), (2, 2)))
    input_proj = centred(seeds[4], (D, GROUPS * STATE), D ** -0.5, 0.125, ((1, 4),))
    output_proj = centred(seeds[5], (D, GROUPS * STATE), D ** -0.5, 0.125, ((1, 4),))
    step_proj = centred(seeds[6], (D, MIXER_HEADS), D ** -0.5, 0.125)
    step_bias = jnp.clip(jax.random.uniform(seeds[7], (MIXER_HEADS,), jnp.float32, -3.0, -0.5), -3.0, -0.5)
    decay_log = jnp.clip(jax.random.uniform(seeds[8], (MIXER_HEADS,), jnp.float32, -3.0, 1.0), -3.0, 1.0)
    skip_gain = jnp.clip(jax.random.uniform(seeds[9], (MIXER_HEADS,), jnp.float32, 0.3, 1.5), 0.3, 1.5)
    taps_inner = centred(seeds[10], (TAPS, MIXER_HEADS, HEAD_DIM), TAPS ** -0.5, 3.0, ((2, 2),), jnp.float32)
    taps_input = centred(seeds[11], (TAPS, GROUPS * STATE), TAPS ** -0.5, 3.0, (), jnp.float32)
    taps_output = centred(seeds[12], (TAPS, GROUPS * STATE), TAPS ** -0.5, 3.0, (), jnp.float32)
    recent_inner = centred(part_keys[13], (GROUP_SEQUENCES, TAPS - 1, MIXER_HEADS, HEAD_DIM), 1.0, 6.0, ((0, 4), (3, 2)))
    recent_input = centred(part_keys[14], (GROUP_SEQUENCES, TAPS - 1, GROUPS * STATE), 1.0, 6.0, ((0, 4),))
    recent_output = centred(part_keys[15], (GROUP_SEQUENCES, TAPS - 1, GROUPS * STATE), 1.0, 6.0, ((0, 4),))
    states = centred(part_keys[16], (GROUP_SEQUENCES, MIXER_HEADS, HEAD_DIM, STATE), 0.3, 4.0, ((0, 4), (2, 2)), jnp.float32)
    block_inner = centred(part_keys[17], (GROUP_SEQUENCES, OPEN_BLOCK_SPAN, MIXER_HEADS, HEAD_DIM), 0.5, 6.0, ((0, 4), (3, 2)))
    block_input = centred(part_keys[18], (GROUP_SEQUENCES, OPEN_BLOCK_SPAN, GROUPS * STATE), 0.25, 4.0, ((0, 4),))
    block_decay = draw_block_decay(jax.random.fold_in(jax.random.fold_in(seeds[27], part), 71), part)
    lengths = uneven_parts(part_keys[20], GROUP_SEQUENCES, GROUP_SEQUENCES * OPEN_BLOCK_SPAN // 3, OPEN_BLOCK_SPAN, 2).astype(jnp.int32)
    norm_gain = jnp.clip(1.0 + 0.18 * jax.random.normal(seeds[21], (MIXER_HEADS, HEAD_DIM), jnp.float32), 0.1, 1.9)
    mixer_out = bell_draw_with(seeds[22], (MIXER_HEADS, HEAD_DIM, D), (MIXER_HEADS * HEAD_DIM) ** -0.5, 0.125, ((0, 4), (1, 2)), (0, 2, 4, 2.0))
    channel_gain = jnp.clip(1.0 + 0.18 * jax.random.normal(seeds[23], (D,), jnp.float32), 0.1, 1.9)
    expand_gate = centred(seeds[24], (D, FF), D ** -0.5, 0.125, ((1, 8),))
    expand_value = centred(seeds[25], (D, FF), D ** -0.5, 0.125, ((1, 8),))
    reduce_proj = bell_draw_with(seeds[26], (FF, D), FF ** -0.5, 0.109375, ((0, 8),), (0, 1, 8, 2.0))
    return {"hidden": hidden, "mixer_gain": mixer_gain, "gate_proj": gate_proj, "inner_proj": inner_proj, "input_proj": input_proj, "output_proj": output_proj, "step_proj": step_proj, "step_bias": step_bias, "decay_log": decay_log, "skip_gain": skip_gain, "taps_inner": taps_inner, "taps_input": taps_input, "taps_output": taps_output, "recent_inner": recent_inner, "recent_input": recent_input, "recent_output": recent_output, "states": states, "block_inner": block_inner, "block_input": block_input, "block_decay": block_decay, "lengths": lengths, "norm_gain": norm_gain, "mixer_out": mixer_out, "channel_gain": channel_gain, "expand_gate": expand_gate, "expand_value": expand_value, "reduce_proj": reduce_proj}


epsilon = 1e-05

def short_conv(recent, newest, taps):
    window = jnp.concatenate([recent.astype(jnp.float32), newest.astype(jnp.float32)[:, None]], axis=1)
    return jax.nn.silu(lax.optimization_barrier(jnp.sum(window * taps[None], axis=1)))

def reference(hidden, mixer_gain, gate_proj, inner_proj, input_proj, output_proj, step_proj, step_bias, decay_log, skip_gain, taps_inner, taps_input, taps_output, recent_inner, recent_input, recent_output, states, block_inner, block_input, block_decay, lengths, norm_gain, mixer_out, channel_gain, expand_gate, expand_value, reduce_proj):
    hidden_f = hidden.astype(jnp.float32)
    rms_in = lax.rsqrt(lax.optimization_barrier(jnp.mean(hidden_f * hidden_f, axis=0)) + epsilon)
    normed_in = (hidden_f * mixer_gain[:, None]).astype(jnp.bfloat16).astype(jnp.float32)
    gate_pre = (rms_in[:, None, None] * jnp.einsum('ds,dhp->shp', normed_in, gate_proj.astype(jnp.float32))).astype(jnp.bfloat16)
    inner_pre = (rms_in[:, None, None] * jnp.einsum('ds,dhp->shp', normed_in, inner_proj.astype(jnp.float32))).astype(jnp.bfloat16)
    input_pre = (rms_in[:, None] * jnp.einsum('ds,dk->sk', normed_in, input_proj.astype(jnp.float32))).astype(jnp.bfloat16)
    output_pre = (rms_in[:, None] * jnp.einsum('ds,dk->sk', normed_in, output_proj.astype(jnp.float32))).astype(jnp.bfloat16)
    step_pre = (rms_in[:, None] * jnp.einsum('ds,dh->sh', normed_in, step_proj.astype(jnp.float32))).astype(jnp.bfloat16)
    conv_inner = short_conv(recent_inner, inner_pre, taps_inner)
    conv_input = short_conv(recent_input, input_pre, taps_input)
    conv_output = short_conv(recent_output, output_pre, taps_output).astype(jnp.bfloat16)
    step = jax.nn.softplus(step_pre.astype(jnp.float32) + step_bias[None, :])
    new_decay = -jnp.exp(decay_log)[None, :] * step
    seq_count = hidden.shape[1]
    per_group = MIXER_HEADS // GROUPS
    live = (jnp.arange(OPEN_BLOCK_SPAN, dtype=jnp.int32)[None, :] < lengths[:, None]).astype(jnp.float32)
    masked = block_decay * live[:, :, None]
    cached = lax.optimization_barrier(jnp.sum(masked, axis=1))
    tail = new_decay[:, None, :] + cached[:, None, :] - jnp.cumsum(masked, axis=1)
    total = new_decay + cached
    readout = conv_output.astype(jnp.float32).reshape(seq_count, GROUPS, STATE)
    score = jnp.einsum('sgn,sjgn->sgj', readout, block_input.astype(jnp.float32).reshape(seq_count, OPEN_BLOCK_SPAN, GROUPS, STATE))
    score_heads = jnp.repeat(score, per_group, axis=1)
    weight = (live[:, None, :] * jnp.exp(jnp.swapaxes(tail, 1, 2)) * score_heads).astype(jnp.bfloat16)
    from_block = jnp.einsum('shj,sjhp->shp', weight.astype(jnp.float32), block_inner.astype(jnp.float32))
    grouped = states.reshape(seq_count, GROUPS, per_group, HEAD_DIM, STATE)
    from_state = jnp.einsum('sgn,sgrpn->sgrp', readout, grouped, precision=lax.Precision.HIGHEST).reshape(seq_count, MIXER_HEADS, HEAD_DIM)
    own_score = jnp.repeat(lax.optimization_barrier(jnp.sum(readout * conv_input.reshape(seq_count, GROUPS, STATE), axis=-1)), per_group, axis=1)
    mix = from_block + jnp.exp(total)[:, :, None] * from_state + (own_score * step)[:, :, None] * conv_inner + skip_gain[None, :, None] * conv_inner
    gated_raw = mix * jax.nn.silu(gate_pre.astype(jnp.float32))
    rms_gate = lax.rsqrt(lax.optimization_barrier(jnp.mean(gated_raw * gated_raw, axis=(1, 2))) + epsilon)
    gated = (gated_raw * norm_gain[None]).astype(jnp.bfloat16)
    mixed = rms_gate[None, :] * jnp.einsum('shp,hpd->ds', gated.astype(jnp.float32), mixer_out.astype(jnp.float32))
    mid = (hidden_f + mixed).astype(jnp.bfloat16).astype(jnp.float32)
    rms_mid = lax.rsqrt(lax.optimization_barrier(jnp.mean(mid * mid, axis=0)) + epsilon)
    normed_mid = (mid * channel_gain[:, None]).astype(jnp.bfloat16).astype(jnp.float32)
    gate_sum = rms_mid[:, None] * jnp.einsum('ds,df->sf', normed_mid, expand_gate.astype(jnp.float32))
    value_sum = rms_mid[:, None] * jnp.einsum('ds,df->sf', normed_mid, expand_value.astype(jnp.float32))
    act = (jax.nn.silu(gate_sum) * value_sum).astype(jnp.bfloat16)
    channel = jnp.einsum('fd,sf->ds', reduce_proj.astype(jnp.float32), act.astype(jnp.float32))
    return (mid + channel).astype(jnp.bfloat16)
```

```python
import functools

import jax
import jax.numpy as jnp
from jax import lax
from jax.experimental import pallas as pl
from jax.experimental.pallas import tpu as pltpu
from jax.sharding import PartitionSpec as P

MIXER_HEADS = 64
HEAD_DIM = 64
GROUPS = 8
STATE = 128
OPEN_BLOCK_SPAN = 128


epsilon = 1e-05


def short_conv(recent, newest, taps):
    window = jnp.concatenate(
        [recent.astype(jnp.float32), newest.astype(jnp.float32)[:, None]], axis=1
    )
    return jax.nn.silu(jnp.sum(window * taps[None], axis=1))


def general(
    hidden,
    mixer_gain,
    gate_proj,
    inner_proj,
    input_proj,
    output_proj,
    step_proj,
    step_bias,
    decay_log,
    skip_gain,
    taps_inner,
    taps_input,
    taps_output,
    recent_inner,
    recent_input,
    recent_output,
    states,
    block_inner,
    block_input,
    block_decay,
    lengths,
    norm_gain,
    mixer_out,
    channel_gain,
    expand_gate,
    expand_value,
    reduce_proj,
):
    rows_own = hidden.shape[0]
    seq_all = hidden.shape[1]
    seq_dev = states.shape[0]
    half_dim = states.shape[2]
    width = rows_own * lax.axis_size("kv") * lax.axis_size("tp")
    offset = (lax.axis_index("kv") * lax.axis_size("tp") + lax.axis_index("tp")) * rows_own
    own_start = lax.axis_index("kv") * seq_dev
    whole_rows = lax.all_gather(hidden, ("kv", "tp"), axis=0, tiled=True)
    whole_f = whole_rows.astype(jnp.float32)
    rms_in = lax.rsqrt(jnp.mean(whole_f * whole_f, axis=0) + epsilon)
    normed_in = (whole_f * mixer_gain[:, None]).astype(jnp.bfloat16)
    gate_part = (
        rms_in[:, None, None]
        * jnp.einsum("ds,dhp->shp", normed_in, gate_proj, preferred_element_type=jnp.float32)
    ).astype(jnp.bfloat16)
    inner_part = (
        rms_in[:, None, None]
        * jnp.einsum("ds,dhp->shp", normed_in, inner_proj, preferred_element_type=jnp.float32)
    ).astype(jnp.bfloat16)
    input_part = (
        rms_in[:, None]
        * jnp.einsum("ds,dk->sk", normed_in, input_proj, preferred_element_type=jnp.float32)
    ).astype(jnp.bfloat16)
    output_part = (
        rms_in[:, None]
        * jnp.einsum("ds,dk->sk", normed_in, output_proj, preferred_element_type=jnp.float32)
    ).astype(jnp.bfloat16)
    own_cols = lax.dynamic_slice_in_dim(normed_in, own_start, seq_dev, 1)
    own_rms = lax.dynamic_slice_in_dim(rms_in, own_start, seq_dev, 0)
    step_pre = (
        own_rms[:, None]
        * jnp.einsum("ds,dh->sh", own_cols, step_proj, preferred_element_type=jnp.float32)
    ).astype(jnp.bfloat16)
    gate_pre, inner_pre, input_pre, output_pre = (
        lax.all_to_all(gate_part, "kv", split_axis=0, concat_axis=1, tiled=True),
        lax.all_to_all(inner_part, "kv", split_axis=0, concat_axis=1, tiled=True),
        lax.all_to_all(input_part, "kv", split_axis=0, concat_axis=1, tiled=True),
        lax.all_to_all(output_part, "kv", split_axis=0, concat_axis=1, tiled=True),
    )
    conv_inner = short_conv(recent_inner, inner_pre, taps_inner)
    conv_input = short_conv(recent_input, input_pre, taps_input)
    conv_output = short_conv(recent_output, output_pre, taps_output).astype(jnp.bfloat16)
    step = jax.nn.softplus(step_pre.astype(jnp.float32) + step_bias[None, :])
    new_decay = -jnp.exp(decay_log)[None, :] * step
    per_group = MIXER_HEADS // GROUPS
    live = (jnp.arange(OPEN_BLOCK_SPAN, dtype=jnp.int32)[None, :] < lengths[:, None]).astype(
        jnp.float32
    )
    masked = block_decay * live[:, :, None]
    cached = jnp.sum(masked, axis=1)
    tail = new_decay[:, None, :] + cached[:, None, :] - jnp.cumsum(masked, axis=1)
    total = new_decay + cached
    readout = conv_output.reshape(seq_dev, GROUPS, STATE)
    score = jnp.einsum(
        "sgn,sjgn->sgj",
        readout,
        block_input.reshape(seq_dev, OPEN_BLOCK_SPAN, GROUPS, STATE),
        preferred_element_type=jnp.float32,
    )
    score_heads = jnp.repeat(score, per_group, axis=1)
    weight = (live[:, None, :] * jnp.exp(jnp.swapaxes(tail, 1, 2)) * score_heads).astype(
        jnp.bfloat16
    )
    from_block = jnp.einsum(
        "shj,sjhp->shp", weight, block_inner, preferred_element_type=jnp.float32
    )
    readout_f = readout.astype(jnp.float32)
    grouped = states.reshape(seq_dev, GROUPS, per_group, half_dim, STATE)
    from_state = jnp.einsum(
        "sgn,sgrpn->sgrp", readout_f, grouped, precision=lax.Precision.HIGHEST
    ).reshape(seq_dev, MIXER_HEADS, half_dim)
    own_score = jnp.repeat(
        jnp.sum(readout_f * conv_input.reshape(seq_dev, GROUPS, STATE), axis=-1), per_group, axis=1
    )
    mix = (
        from_block
        + jnp.exp(total)[:, :, None] * from_state
        + (own_score * step)[:, :, None] * conv_inner
        + skip_gain[None, :, None] * conv_inner
    )
    gated_raw = mix * jax.nn.silu(gate_pre.astype(jnp.float32))
    part_squares = jnp.sum(gated_raw * gated_raw, axis=(1, 2))
    gated = (gated_raw * norm_gain[None]).astype(jnp.bfloat16)
    placed = lax.dynamic_update_slice_in_dim(
        jnp.zeros((seq_all,), jnp.float32), part_squares, own_start, 0
    )
    gate_squares = lax.psum(placed, ("kv", "tp"))
    rms_gate = lax.rsqrt(gate_squares / (MIXER_HEADS * HEAD_DIM) + epsilon)
    by_head = lax.all_to_all(gated, "kv", split_axis=1, concat_axis=0, tiled=True)
    columns = mixer_out
    mixed_full = rms_gate[None, :] * lax.psum(
        jnp.einsum("hpd,shp->ds", columns, by_head, preferred_element_type=jnp.float32),
        ("kv", "tp"),
    )
    mid_full = (whole_f + mixed_full).astype(jnp.bfloat16)
    mid = lax.dynamic_slice_in_dim(mid_full, offset, rows_own, 0)
    full_f = mid_full.astype(jnp.float32)
    mid_squares = jnp.sum(full_f * full_f, axis=0)
    normed_full = (full_f * channel_gain[:, None]).astype(jnp.bfloat16)
    gate_sum = jnp.einsum("ds,df->sf", normed_full, expand_gate, preferred_element_type=jnp.float32)
    value_sum = jnp.einsum(
        "ds,df->sf", normed_full, expand_value, preferred_element_type=jnp.float32
    )
    rms_mid = lax.rsqrt(mid_squares / width + epsilon)
    act = (jax.nn.silu(rms_mid[:, None] * gate_sum) * (rms_mid[:, None] * value_sum)).astype(
        jnp.bfloat16
    )
    columns = reduce_proj
    channel = lax.psum_scatter(
        jnp.einsum("fd,sf->ds", columns, act, preferred_element_type=jnp.float32),
        ("kv", "tp"),
        scatter_dimension=0,
        tiled=True,
    )
    return (mid.astype(jnp.float32) + channel).astype(jnp.bfloat16)


NT = (((1,), (1,)), ((), ()))
NN = (((1,), (0,)), ((), ()))
LANES = 128


def dot(a, b, dims, precision=None):
    return lax.dot_general(a, b, dims, precision=precision, preferred_element_type=jnp.float32)


def silu(v):
    return v / (1.0 + jnp.exp(-v))


def tree(values):
    values = list(values)
    while len(values) > 1:
        values = [a + b for a, b in zip(values[::2], values[1::2])]
    return values[0]


def call(body, outs, args, scratch=(), scalars=(), flops=0):
    args = [
        a if i in scalars else pltpu.with_memory_space_constraint(a, pltpu.VMEM)
        for i, a in enumerate(args)
    ]
    return pl.pallas_call(
        body,
        out_shape=[pltpu.VMEM(s, d) for s, d in outs],
        in_specs=[
            pl.BlockSpec(memory_space=pltpu.SMEM if i in scalars else pltpu.VMEM)
            for i in range(len(args))
        ],
        out_specs=[pl.BlockSpec(memory_space=pltpu.VMEM) for _ in outs],
        scratch_shapes=[pltpu.VMEM(s, d) for s, d in scratch],
        compiler_params=pltpu.CompilerParams(vmem_limit_bytes=8 << 20),
        cost_estimate=pl.CostEstimate(flops=flops, bytes_accessed=0, transcendentals=0),
    )(*args)


def lane(start, size):
    return pl.ds(pl.multiple_of(start, LANES), size)


def project(n, *refs):
    pieces, refs = refs[:n], refs[n:]
    mixer_gain, gate_w, inner_w, input_w, output_w, step_w = refs[:6]
    x_out, step_out = refs[6:8]
    sends = refs[8:]
    kv, tp = lax.axis_index("kv"), lax.axis_index("tp")
    width = x_out.shape[1]
    part = pieces[0].shape[1] // 2
    for k, ref in enumerate(pieces):
        base = (kv ^ k) * (2 * part)
        x_out[:, lane(base + tp * part, part)] = ref[:, :part]
        x_out[:, lane(base + (1 - tp) * part, part)] = ref[:, part:]
    x = x_out[...].astype(jnp.float32)
    rms = lax.rsqrt(jnp.sum(x * x, axis=1, keepdims=True) / width + epsilon)
    normed = (x * mixer_gain[...]).astype(jnp.bfloat16)
    at = 0
    for weight, dims in ((gate_w, NT), (inner_w, NT), (input_w, NN), (output_w, NN)):
        value = rms * dot(normed, weight[...], dims)
        value = value.astype(jnp.bfloat16).astype(jnp.float32)
        row = lax.broadcasted_iota(jnp.int32, value.shape, 0)
        for k, ref in enumerate(sends):
            picked = jnp.sum(jnp.where(row == (kv ^ k), value, 0.0), axis=0, keepdims=True)
            ref[:, at : at + value.shape[1]] = picked
        at += value.shape[1]
    steps = (rms * dot(normed, step_w[...], NT)).astype(jnp.bfloat16).astype(jnp.float32)
    row = lax.broadcasted_iota(jnp.int32, steps.shape, 0)
    step_out[...] = jnp.sum(jnp.where(row == kv, steps, 0.0), axis=0, keepdims=True)


def mixer(n, length, *refs):
    pieces, refs = refs[:n], refs[n:]
    step_pre, step_bias, decay_log, skip_gain = refs[:4]
    taps_inner, taps_input, taps_output = refs[4:7]
    recent_inner, recent_input, recent_output = refs[7:10]
    states, block_inner, block_input, block_decay, norm_gain = refs[10:15]
    sends, (gate_row, inner_row, input_row, output_row, gated_row) = refs[15:-5], refs[-5:]
    kv = lax.axis_index("kv")
    heads, span = block_decay.shape
    channels = gate_row.shape[1]
    half = channels // heads
    size = states.shape[1]
    groups = block_input.shape[1] // size
    per_group = heads // groups
    chunk = per_group * half
    cols, maps = channels // n, input_row.shape[1] // n
    for k, ref in enumerate(pieces):
        src = kv ^ k
        gate_row[:, lane(src * cols, cols)] = ref[:, :cols]
        inner_row[:, lane(src * cols, cols)] = ref[:, cols : 2 * cols]
        input_row[:, lane(src * maps, maps)] = ref[:, 2 * cols : 2 * cols + maps]
        output_row[:, lane(src * maps, maps)] = ref[:, 2 * cols + maps :]

    def conv(recent, newest, taps):
        weights = taps[...]
        past = jnp.sum(recent[...].astype(jnp.float32) * weights[:-1], axis=0, keepdims=True)
        return silu(past + weights[-1:] * newest)

    conv_output = conv(recent_output, output_row[...], taps_output).astype(jnp.bfloat16)
    conv_input = conv(recent_input, input_row[...], taps_input)
    conv_inner = conv(recent_inner, inner_row[...], taps_inner)
    readout = conv_output.astype(jnp.float32)

    eye = lax.broadcasted_iota(jnp.int32, (heads, heads), 0) == lax.broadcasted_iota(
        jnp.int32, (heads, heads), 1
    )

    def column(row):
        return jnp.sum(jnp.where(eye, row, 0.0), axis=1, keepdims=True)

    pre = step_pre[...] + step_bias[...]
    step_row = jnp.maximum(pre, 0.0) + jnp.log1p(jnp.exp(-jnp.abs(pre)))
    step = column(step_row)
    new_decay = column(-jnp.exp(decay_log[...]) * step_row)
    skip = column(skip_gain[...])

    live = (lax.broadcasted_iota(jnp.int32, (1, span), 1) < length[0]).astype(jnp.float32)
    masked = block_decay[...] * live
    later = (
        lax.broadcasted_iota(jnp.int32, (span, span), 0)
        > lax.broadcasted_iota(jnp.int32, (span, span), 1)
    ).astype(jnp.float32)
    suffix = dot(masked, later, NN, lax.Precision.HIGHEST)
    grown = jnp.exp(new_decay + jnp.sum(masked, axis=1, keepdims=True))
    decayed = live * jnp.exp(new_decay + suffix)

    wide = (groups, groups * size)
    diagonal = lax.broadcasted_iota(jnp.int32, wide, 1) // size == lax.broadcasted_iota(
        jnp.int32, wide, 0
    )
    spread = jnp.where(diagonal, readout, 0.0)
    score = dot(spread.astype(jnp.bfloat16), block_input[...], NT)
    own_score = jnp.sum(spread * conv_input, axis=1, keepdims=True)

    narrow = (per_group, chunk)
    mine = lax.broadcasted_iota(jnp.int32, narrow, 1) // half == lax.broadcasted_iota(
        jnp.int32, narrow, 0
    )
    squares = jnp.zeros((1, chunk), jnp.float32)
    for g in range(groups):
        head = slice(g * per_group, (g + 1) * per_group)
        rows = slice(g * chunk, (g + 1) * chunk)
        weight = (decayed[head] * score[g : g + 1]).astype(jnp.bfloat16)
        from_block = dot(weight, block_inner[rows, :], NT)
        state = states[rows, :]
        high = state.astype(jnp.bfloat16)
        low = (state - high.astype(jnp.float32)).astype(jnp.bfloat16)
        out_map = jnp.broadcast_to(
            readout[:, g * size : (g + 1) * size], (per_group, size)
        ).astype(jnp.bfloat16)
        from_state = dot(out_map, high, NT) + dot(out_map, low, NT)
        direct = own_score[g : g + 1] * step[head] + skip[head]
        both = from_block + grown[head] * from_state + direct * conv_inner[:, rows]
        mix = jnp.sum(jnp.where(mine, both, 0.0), axis=0, keepdims=True)
        raw = mix * silu(gate_row[:, rows])
        squares = squares + raw * raw
        gated_row[:, rows] = (raw * norm_gain[:, rows]).astype(jnp.bfloat16).astype(jnp.float32)
    square = jnp.sum(squares, axis=1, keepdims=True)
    for k, ref in enumerate(sends):
        ref[:, :cols] = gated_row[:, lane((kv ^ k) * cols, cols)]
        ref[:, cols:] = jnp.broadcast_to(square, (1, LANES))


def out_project(n, *refs):
    pieces, (mixer_out, out, rows) = refs[:n], refs[n:]
    kv = lax.axis_index("kv")
    cols, width = mixer_out.shape
    for k, ref in enumerate(pieces):
        rows[pl.ds(kv ^ k, 1), :] = ref[...]
    out[:, :width] = dot(rows[:, :cols].astype(jnp.bfloat16), mixer_out[...], NN)
    out[:, width:] = rows[:, cols:]


def add_pair(a, b, out):
    out[...] = a[...] + b[...]


def channel_mix(n, channels, *refs):
    pieces, (x, gain, gate_w, value_w, reduce_w) = refs[:n], refs[n : n + 5]
    mid_out, keep, send, moved = refs[n + 5 :]
    kv, tp = lax.axis_index("kv"), lax.axis_index("tp")
    width = x.shape[1]
    part = mid_out.shape[1]
    whole = tree(ref[:, :width] for ref in pieces)
    rms_gate = lax.rsqrt(pieces[0][:, width : width + 1] / channels + epsilon)
    mid = (x[...].astype(jnp.float32) + rms_gate * whole).astype(jnp.bfloat16)
    mid = mid.astype(jnp.float32)
    rms = lax.rsqrt(jnp.sum(mid * mid, axis=1, keepdims=True) / width + epsilon)
    normed = (mid * gain[...]).astype(jnp.bfloat16)
    moved[...] = mid
    mid_out[...] = moved[:, lane((kv * 2 + tp) * part, part)]
    act = silu(rms * dot(normed, gate_w[...], NT)) * (rms * dot(normed, value_w[...], NT))
    moved[...] = dot(act.astype(jnp.bfloat16), reduce_w[...], NN)
    for i in range(n):
        at = slice(i * part, (i + 1) * part)
        keep[:, at] = moved[:, lane((2 * i + tp) * part, part)]
        send[:, at] = moved[:, lane((2 * i + 1 - tp) * part, part)]


def split_pair(n, a, b, *outs):
    *outs, moved = outs
    kv = lax.axis_index("kv")
    part = outs[0].shape[1]
    moved[...] = a[...] + b[...]
    for k, ref in enumerate(outs):
        ref[...] = moved[:, lane((kv ^ k) * part, part)]


def finish(n, *refs):
    pieces, (mid, out) = refs[:n], refs[n:]
    out[...] = (mid[...] + tree(ref[...] for ref in pieces)).astype(jnp.bfloat16)


def across(label, values):
    n = len(values)
    got = [values[0]] + [None] * (n - 1)
    for k in reversed(range(1, n)):
        with jax.named_scope(f"{label}_{k}"):
            got[k] = lax.ppermute(values[k], "kv", [(i, i ^ k) for i in range(n)])
    return got


def beside(label, value):
    with jax.named_scope(label):
        return lax.ppermute(value, "tp", [(0, 1), (1, 0)])


def layer(*args):
    (
        hidden, mixer_gain, gate_proj, inner_proj, input_proj, output_proj, step_proj, step_bias,
        decay_log, skip_gain, taps_inner, taps_input, taps_output, recent_inner, recent_input,
        recent_output, states, block_inner, block_input, block_decay, lengths, norm_gain, mixer_out,
        channel_gain, expand_gate, expand_value, reduce_proj,
    ) = args
    n = lax.axis_size("kv")
    part, seqs = hidden.shape
    width = part * n * 2
    heads, half, size = states.shape[1:]
    channels = heads * half
    cols, maps = channels // n, input_proj.shape[1]
    aligned = all(v % LANES == 0 for v in (part, cols, maps, width, size, block_decay.shape[1]))
    if not (
        n & (n - 1) == 0
        and lax.axis_size("tp") == 2
        and states.shape[0] == 1
        and seqs == n
        and aligned
    ):
        return general(*args)
    f32, bf16 = jnp.float32, jnp.bfloat16
    x = hidden.T
    pair = jnp.concatenate([x, beside("in_tp", x)], axis=1)
    pieces = across("in", [pair] * n)
    whole, step_pre, *sends = call(
        functools.partial(project, n),
        [((seqs, width), bf16), ((1, heads), f32)] + [((1, 2 * cols + 2 * maps), f32)] * n,
        pieces
        + [
            mixer_gain.reshape(1, width),
            gate_proj.transpose(1, 2, 0).reshape(cols, width),
            inner_proj.transpose(1, 2, 0).reshape(cols, width),
            input_proj,
            output_proj,
            step_proj.T,
        ],
        flops=2 * seqs * width * (2 * cols + 2 * maps),
    )
    pieces = across("pre", sends)
    sends = call(
        functools.partial(mixer, n),
        [((1, cols + LANES), f32)] * n,
        [lengths]
        + pieces
        + [
            step_pre,
            step_bias.reshape(1, heads),
            decay_log.reshape(1, heads),
            skip_gain.reshape(1, heads),
            taps_inner.reshape(-1, channels),
            taps_input,
            taps_output,
            recent_inner.reshape(-1, channels),
            recent_input[0],
            recent_output[0],
            states.reshape(channels, size),
            block_inner.transpose(0, 2, 3, 1).reshape(channels, -1),
            block_input[0],
            block_decay[0].T,
            norm_gain.reshape(1, channels),
        ],
        scratch=[((1, channels), f32)] * 2 + [((1, n * maps), f32)] * 2 + [((1, channels), f32)],
        scalars=(0,),
        flops=1 << 24,
    )
    pieces = across("gated", sends)
    (mixed,) = call(
        functools.partial(out_project, n),
        [((seqs, width + LANES), f32)],
        pieces + [mixer_out.reshape(cols, width)],
        scratch=[((seqs, cols + LANES), f32)],
        flops=2 * seqs * width * cols,
    )
    (mixed,) = call(
        add_pair, [((seqs, width + LANES), f32)], [mixed, beside("mixed_tp", mixed)]
    )
    pieces = across("mixed", [mixed] * n)
    mid, keep, send = call(
        functools.partial(channel_mix, n, 2 * channels),
        [((seqs, part), f32)] + [((seqs, width // 2), f32)] * 2,
        pieces
        + [whole, channel_gain.reshape(1, width), expand_gate.T, expand_value.T, reduce_proj],
        scratch=[((seqs, width), f32)],
        flops=6 * seqs * width * reduce_proj.shape[0],
    )
    sends = call(
        functools.partial(split_pair, n),
        [((seqs, part), f32)] * n,
        [keep, beside("down_tp", send)],
        scratch=[((seqs, width // 2), f32)],
    )
    pieces = across("down", sends)
    (out,) = call(functools.partial(finish, n), [((seqs, part), bf16)], pieces + [mid])
    return out.T


def solution(mesh):
    return jax.shard_map(
        layer,
        mesh=mesh,
        in_specs=(
            P(("kv", "tp"), "dp"),
            P(),
            P(None, "kv", "tp"),
            P(None, "kv", "tp"),
            P(None, "kv"),
            P(None, "kv"),
            P(),
            P(),
            P(),
            P(),
            P(None, None, "tp"),
            P(),
            P(),
            P(("dp", "kv"), None, None, "tp"),
            P(("dp", "kv"), None, None),
            P(("dp", "kv"), None, None),
            P(("dp", "kv"), None, "tp", None),
            P(("dp", "kv"), None, None, "tp"),
            P(("dp", "kv"), None, None),
            P(("dp", "kv"), None, None),
            P(("dp", "kv")),
            P(None, "tp"),
            P("kv", "tp", None),
            P(),
            P(None, ("kv", "tp")),
            P(None, ("kv", "tp")),
            P(("kv", "tp"), None),
        ),
        out_specs=P(("kv", "tp"), "dp"),
        check_vma=False,
    )
```

```python
import functools

import jax
import jax.numpy as jnp
from jax import lax
from jax.experimental import pallas as pl
from jax.experimental.pallas import tpu as pltpu
from jax.sharding import PartitionSpec as P


MIXER_HEADS = 64
HEAD_DIM = 64
GROUPS = 8
STATE = 128
OPEN_BLOCK_SPAN = 128


epsilon = 1e-05


def short_conv(recent, newest, taps):
    window = jnp.concatenate(
        [recent.astype(jnp.float32), newest.astype(jnp.float32)[:, None]], axis=1
    )
    return jax.nn.silu(jnp.sum(window * taps[None], axis=1))


def general(
    hidden,
    mixer_gain,
    gate_proj,
    inner_proj,
    input_proj,
    output_proj,
    step_proj,
    step_bias,
    decay_log,
    skip_gain,
    taps_inner,
    taps_input,
    taps_output,
    recent_inner,
    recent_input,
    recent_output,
    states,
    block_inner,
    block_input,
    block_decay,
    lengths,
    norm_gain,
    mixer_out,
    channel_gain,
    expand_gate,
    expand_value,
    reduce_proj,
):
    rows_own = hidden.shape[0]
    seq_all = hidden.shape[1]
    seq_dev = states.shape[0]
    half_dim = states.shape[2]
    width = rows_own * lax.axis_size("kv") * lax.axis_size("tp")
    offset = (lax.axis_index("kv") * lax.axis_size("tp") + lax.axis_index("tp")) * rows_own
    own_start = lax.axis_index("kv") * seq_dev
    whole_rows = lax.all_gather(hidden, ("kv", "tp"), axis=0, tiled=True)
    whole_f = whole_rows.astype(jnp.float32)
    rms_in = lax.rsqrt(jnp.mean(whole_f * whole_f, axis=0) + epsilon)
    normed_in = (whole_f * mixer_gain[:, None]).astype(jnp.bfloat16)
    gate_part = (
        rms_in[:, None, None]
        * jnp.einsum("ds,dhp->shp", normed_in, gate_proj, preferred_element_type=jnp.float32)
    ).astype(jnp.bfloat16)
    inner_part = (
        rms_in[:, None, None]
        * jnp.einsum("ds,dhp->shp", normed_in, inner_proj, preferred_element_type=jnp.float32)
    ).astype(jnp.bfloat16)
    input_part = (
        rms_in[:, None]
        * jnp.einsum("ds,dk->sk", normed_in, input_proj, preferred_element_type=jnp.float32)
    ).astype(jnp.bfloat16)
    output_part = (
        rms_in[:, None]
        * jnp.einsum("ds,dk->sk", normed_in, output_proj, preferred_element_type=jnp.float32)
    ).astype(jnp.bfloat16)
    own_cols = lax.dynamic_slice_in_dim(normed_in, own_start, seq_dev, 1)
    own_rms = lax.dynamic_slice_in_dim(rms_in, own_start, seq_dev, 0)
    step_pre = (
        own_rms[:, None]
        * jnp.einsum("ds,dh->sh", own_cols, step_proj, preferred_element_type=jnp.float32)
    ).astype(jnp.bfloat16)
    gate_pre, inner_pre, input_pre, output_pre = (
        lax.all_to_all(gate_part, "kv", split_axis=0, concat_axis=1, tiled=True),
        lax.all_to_all(inner_part, "kv", split_axis=0, concat_axis=1, tiled=True),
        lax.all_to_all(input_part, "kv", split_axis=0, concat_axis=1, tiled=True),
        lax.all_to_all(output_part, "kv", split_axis=0, concat_axis=1, tiled=True),
    )
    conv_inner = short_conv(recent_inner, inner_pre, taps_inner)
    conv_input = short_conv(recent_input, input_pre, taps_input)
    conv_output = short_conv(recent_output, output_pre, taps_output).astype(jnp.bfloat16)
    step = jax.nn.softplus(step_pre.astype(jnp.float32) + step_bias[None, :])
    new_decay = -jnp.exp(decay_log)[None, :] * step
    per_group = MIXER_HEADS // GROUPS
    live = (jnp.arange(OPEN_BLOCK_SPAN, dtype=jnp.int32)[None, :] < lengths[:, None]).astype(
        jnp.float32
    )
    masked = block_decay * live[:, :, None]
    cached = jnp.sum(masked, axis=1)
    tail = new_decay[:, None, :] + cached[:, None, :] - jnp.cumsum(masked, axis=1)
    total = new_decay + cached
    readout = conv_output.reshape(seq_dev, GROUPS, STATE)
    score = jnp.einsum(
        "sgn,sjgn->sgj",
        readout,
        block_input.reshape(seq_dev, OPEN_BLOCK_SPAN, GROUPS, STATE),
        preferred_element_type=jnp.float32,
    )
    score_heads = jnp.repeat(score, per_group, axis=1)
    weight = (live[:, None, :] * jnp.exp(jnp.swapaxes(tail, 1, 2)) * score_heads).astype(
        jnp.bfloat16
    )
    from_block = jnp.einsum(
        "shj,sjhp->shp", weight, block_inner, preferred_element_type=jnp.float32
    )
    readout_f = readout.astype(jnp.float32)
    grouped = states.reshape(seq_dev, GROUPS, per_group, half_dim, STATE)
    from_state = jnp.einsum(
        "sgn,sgrpn->sgrp", readout_f, grouped, precision=lax.Precision.HIGHEST
    ).reshape(seq_dev, MIXER_HEADS, half_dim)
    own_score = jnp.repeat(
        jnp.sum(readout_f * conv_input.reshape(seq_dev, GROUPS, STATE), axis=-1), per_group, axis=1
    )
    mix = (
        from_block
        + jnp.exp(total)[:, :, None] * from_state
        + (own_score * step)[:, :, None] * conv_inner
        + skip_gain[None, :, None] * conv_inner
    )
    gated_raw = mix * jax.nn.silu(gate_pre.astype(jnp.float32))
    part_squares = jnp.sum(gated_raw * gated_raw, axis=(1, 2))
    gated = (gated_raw * norm_gain[None]).astype(jnp.bfloat16)
    placed = lax.dynamic_update_slice_in_dim(
        jnp.zeros((seq_all,), jnp.float32), part_squares, own_start, 0
    )
    gate_squares = lax.psum(placed, ("kv", "tp"))
    rms_gate = lax.rsqrt(gate_squares / (MIXER_HEADS * HEAD_DIM) + epsilon)
    by_head = lax.all_to_all(gated, "kv", split_axis=1, concat_axis=0, tiled=True)
    columns = mixer_out
    mixed_full = rms_gate[None, :] * lax.psum(
        jnp.einsum("hpd,shp->ds", columns, by_head, preferred_element_type=jnp.float32),
        ("kv", "tp"),
    )
    mid_full = (whole_f + mixed_full).astype(jnp.bfloat16)
    mid = lax.dynamic_slice_in_dim(mid_full, offset, rows_own, 0)
    full_f = mid_full.astype(jnp.float32)
    mid_squares = jnp.sum(full_f * full_f, axis=0)
    normed_full = (full_f * channel_gain[:, None]).astype(jnp.bfloat16)
    gate_sum = jnp.einsum("ds,df->sf", normed_full, expand_gate, preferred_element_type=jnp.float32)
    value_sum = jnp.einsum(
        "ds,df->sf", normed_full, expand_value, preferred_element_type=jnp.float32
    )
    rms_mid = lax.rsqrt(mid_squares / width + epsilon)
    act = (jax.nn.silu(rms_mid[:, None] * gate_sum) * (rms_mid[:, None] * value_sum)).astype(
        jnp.bfloat16
    )
    columns = reduce_proj
    channel = lax.psum_scatter(
        jnp.einsum("fd,sf->ds", columns, act, preferred_element_type=jnp.float32),
        ("kv", "tp"),
        scatter_dimension=0,
        tiled=True,
    )
    return (mid.astype(jnp.float32) + channel).astype(jnp.bfloat16)


NT = (((1,), (1,)), ((), ()))
NN = (((1,), (0,)), ((), ()))
LANES = 128


def dot(a, b, dims, precision=None):
    return lax.dot_general(a, b, dims, precision=precision, preferred_element_type=jnp.float32)


def silu(v):
    return v / (1.0 + jnp.exp(-v))


def tree(values):
    values = list(values)
    while len(values) > 1:
        values = [a + b for a, b in zip(values[::2], values[1::2])]
    return values[0]


def call(body, outs, args, scratch=(), scalars=()):
    args = [
        a if i in scalars else pltpu.with_memory_space_constraint(a, pltpu.VMEM)
        for i, a in enumerate(args)
    ]
    return pl.pallas_call(
        body,
        out_shape=[pltpu.VMEM(s, d) for s, d in outs],
        in_specs=[
            pl.BlockSpec(memory_space=pltpu.SMEM if i in scalars else pltpu.VMEM)
            for i in range(len(args))
        ],
        out_specs=[pl.BlockSpec(memory_space=pltpu.VMEM) for _ in outs],
        scratch_shapes=[pltpu.VMEM(s, d) for s, d in scratch],
        compiler_params=pltpu.CompilerParams(vmem_limit_bytes=8 << 20),
        cost_estimate=pl.CostEstimate(flops=20_000_000_000, bytes_accessed=0, transcendentals=0),
    )(*args)


def lane(start, size):
    return pl.ds(pl.multiple_of(start, LANES), size)


def hold(a, out):
    out[...] = a[...]


def stack(a, b, out):
    part = a.shape[1]
    out[:, :part] = a[...]
    out[:, part:] = b[...]


def project(n, *refs):
    pieces, refs = refs[:n], refs[n:]
    mixer_gain, gate_w, inner_w, input_w, output_w, step_w = refs[:6]
    x_out, step_out = refs[6:8]
    sends = refs[8:]
    kv, tp = lax.axis_index("kv"), lax.axis_index("tp")
    width = x_out.shape[1]
    part = pieces[0].shape[1] // 2
    for k, ref in enumerate(pieces):
        base = (kv ^ k) * (2 * part)
        x_out[:, lane(base + tp * part, part)] = ref[:, :part]
        x_out[:, lane(base + (1 - tp) * part, part)] = ref[:, part:]
    x = x_out[...].astype(jnp.float32)
    rms = lax.rsqrt(jnp.sum(x * x, axis=1, keepdims=True) / width + epsilon)
    normed = (x * mixer_gain[...]).astype(jnp.bfloat16)
    at = 0
    for weight, dims in ((gate_w, NT), (inner_w, NT), (input_w, NN), (output_w, NN)):
        value = rms * dot(normed, weight[...], dims)
        value = value.astype(jnp.bfloat16).astype(jnp.float32)
        row = lax.broadcasted_iota(jnp.int32, value.shape, 0)
        for k, ref in enumerate(sends):
            picked = jnp.sum(jnp.where(row == (kv ^ k), value, 0.0), axis=0, keepdims=True)
            ref[:, at : at + value.shape[1]] = picked
        at += value.shape[1]
    steps = (rms * dot(normed, step_w[...], NT)).astype(jnp.bfloat16).astype(jnp.float32)
    row = lax.broadcasted_iota(jnp.int32, steps.shape, 0)
    step_out[...] = jnp.sum(jnp.where(row == kv, steps, 0.0), axis=0, keepdims=True)


def mixer(n, length, *refs):
    pieces, refs = refs[:n], refs[n:]
    step_pre, step_bias, decay_log, skip_gain = refs[:4]
    taps_inner, taps_input, taps_output = refs[4:7]
    recent_inner, recent_input, recent_output = refs[7:10]
    states, block_inner, block_input, block_decay, norm_gain = refs[10:15]
    sends, (gate_row, inner_row, input_row, output_row, gated_row) = refs[15:-5], refs[-5:]
    kv = lax.axis_index("kv")
    heads, span = block_decay.shape
    channels = gate_row.shape[1]
    half = channels // heads
    size = states.shape[1]
    groups = block_input.shape[1] // size
    per_group = heads // groups
    chunk = per_group * half
    cols, maps = channels // n, input_row.shape[1] // n
    for k, ref in enumerate(pieces):
        src = kv ^ k
        gate_row[:, lane(src * cols, cols)] = ref[:, :cols]
        inner_row[:, lane(src * cols, cols)] = ref[:, cols : 2 * cols]
        input_row[:, lane(src * maps, maps)] = ref[:, 2 * cols : 2 * cols + maps]
        output_row[:, lane(src * maps, maps)] = ref[:, 2 * cols + maps :]

    def conv(recent, newest, taps):
        weights = taps[...]
        past = jnp.sum(recent[...].astype(jnp.float32) * weights[:-1], axis=0, keepdims=True)
        return silu(past + weights[-1:] * newest)

    conv_output = conv(recent_output, output_row[...], taps_output).astype(jnp.bfloat16)
    conv_input = conv(recent_input, input_row[...], taps_input)
    conv_inner = conv(recent_inner, inner_row[...], taps_inner)
    readout = conv_output.astype(jnp.float32)

    eye = lax.broadcasted_iota(jnp.int32, (heads, heads), 0) == lax.broadcasted_iota(
        jnp.int32, (heads, heads), 1
    )

    def column(row):
        return jnp.sum(jnp.where(eye, row, 0.0), axis=1, keepdims=True)

    pre = step_pre[...] + step_bias[...]
    step_row = jnp.maximum(pre, 0.0) + jnp.log1p(jnp.exp(-jnp.abs(pre)))
    step = column(step_row)
    new_decay = column(-jnp.exp(decay_log[...]) * step_row)
    skip = column(skip_gain[...])

    live = (lax.broadcasted_iota(jnp.int32, (1, span), 1) < length[0]).astype(jnp.float32)
    masked = block_decay[...] * live
    later = (
        lax.broadcasted_iota(jnp.int32, (span, span), 0)
        > lax.broadcasted_iota(jnp.int32, (span, span), 1)
    ).astype(jnp.float32)
    suffix = dot(masked, later, NN, lax.Precision.HIGHEST)
    grown = jnp.exp(new_decay + jnp.sum(masked, axis=1, keepdims=True))
    decayed = live * jnp.exp(new_decay + suffix)

    wide = (groups, groups * size)
    diagonal = lax.broadcasted_iota(jnp.int32, wide, 1) // size == lax.broadcasted_iota(
        jnp.int32, wide, 0
    )
    spread = jnp.where(diagonal, readout, 0.0)
    score = dot(spread.astype(jnp.bfloat16), block_input[...], NT)
    own_score = jnp.sum(spread * conv_input, axis=1, keepdims=True)

    narrow = (per_group, chunk)
    mine = lax.broadcasted_iota(jnp.int32, narrow, 1) // half == lax.broadcasted_iota(
        jnp.int32, narrow, 0
    )
    squares = jnp.zeros((1, chunk), jnp.float32)
    for g in range(groups):
        head = slice(g * per_group, (g + 1) * per_group)
        rows = slice(g * chunk, (g + 1) * chunk)
        weight = (decayed[head] * score[g : g + 1]).astype(jnp.bfloat16)
        from_block = dot(weight, block_inner[rows, :], NT)
        state = states[rows, :]
        high = state.astype(jnp.bfloat16)
        low = (state - high.astype(jnp.float32)).astype(jnp.bfloat16)
        out_map = jnp.broadcast_to(
            readout[:, g * size : (g + 1) * size], (per_group, size)
        ).astype(jnp.bfloat16)
        from_state = dot(out_map, high, NT) + dot(out_map, low, NT)
        direct = own_score[g : g + 1] * step[head] + skip[head]
        both = from_block + grown[head] * from_state + direct * conv_inner[:, rows]
        mix = jnp.sum(jnp.where(mine, both, 0.0), axis=0, keepdims=True)
        raw = mix * silu(gate_row[:, rows])
        squares = squares + raw * raw
        gated_row[:, rows] = (raw * norm_gain[:, rows]).astype(jnp.bfloat16).astype(jnp.float32)
    square = jnp.sum(squares, axis=1, keepdims=True)
    for k, ref in enumerate(sends):
        ref[:, :cols] = gated_row[:, lane((kv ^ k) * cols, cols)]
        ref[:, cols:] = jnp.broadcast_to(square, (1, LANES))


def out_project(n, *refs):
    pieces, (mixer_out, out, rows) = refs[:n], refs[n:]
    kv = lax.axis_index("kv")
    cols, width = mixer_out.shape
    for k, ref in enumerate(pieces):
        rows[pl.ds(kv ^ k, 1), :] = ref[...]
    out[:, :width] = dot(rows[:, :cols].astype(jnp.bfloat16), mixer_out[...], NN)
    out[:, width:] = rows[:, cols:]


def add_pair(a, b, out, squares):
    width = out.shape[1]
    out[...] = (a[:, :width] + b[:, :width]).astype(jnp.bfloat16)
    squares[...] = a[:, width:] + b[:, width:]


def channel_mix(n, channels, *refs):
    pieces, (squares, x, gain, gate_w, value_w, reduce_w) = refs[:n], refs[n : n + 6]
    mid_out, keep, send, moved = refs[n + 6 :]
    kv, tp = lax.axis_index("kv"), lax.axis_index("tp")
    width = x.shape[1]
    part = mid_out.shape[1]
    whole = tree(ref[...].astype(jnp.float32) for ref in pieces)
    rms_gate = lax.rsqrt(squares[:, :1] / channels + epsilon)
    mid = (x[...].astype(jnp.float32) + rms_gate * whole).astype(jnp.bfloat16)
    mid = mid.astype(jnp.float32)
    rms = lax.rsqrt(jnp.sum(mid * mid, axis=1, keepdims=True) / width + epsilon)
    normed = (mid * gain[...]).astype(jnp.bfloat16)
    moved[...] = mid
    mid_out[...] = moved[:, lane((kv * 2 + tp) * part, part)]
    act = silu(rms * dot(normed, gate_w[...], NT)) * (rms * dot(normed, value_w[...], NT))
    moved[...] = dot(act.astype(jnp.bfloat16), reduce_w[...], NN)
    for i in range(n):
        at = slice(i * part, (i + 1) * part)
        keep[:, at] = moved[:, lane((2 * i + tp) * part, part)]
        send[:, at] = moved[:, lane((2 * i + 1 - tp) * part, part)]


def split_pair(a, b, *outs):
    *outs, moved = outs
    kv = lax.axis_index("kv")
    part = outs[0].shape[1]
    moved[...] = a[...] + b[...]
    for k, ref in enumerate(outs):
        ref[...] = moved[:, lane((kv ^ k) * part, part)]


def finish(n, *refs):
    pieces, (mid, out) = refs[:n], refs[n:]
    out[...] = (mid[...] + tree(ref[...] for ref in pieces)).astype(jnp.bfloat16)


def across(values):
    n = len(values)
    got = [values[0]] + [None] * (n - 1)
    for k in range(1, n):
        got[k] = lax.ppermute(values[k], "kv", [(i, i ^ k) for i in range(n)])
    return got


def beside(value):
    return lax.ppermute(value, "tp", [(0, 1), (1, 0)])


def layer(*args):
    (
        hidden, mixer_gain, gate_proj, inner_proj, input_proj, output_proj, step_proj, step_bias,
        decay_log, skip_gain, taps_inner, taps_input, taps_output, recent_inner, recent_input,
        recent_output, states, block_inner, block_input, block_decay, lengths, norm_gain, mixer_out,
        channel_gain, expand_gate, expand_value, reduce_proj,
    ) = args
    n = lax.axis_size("kv")
    part, seqs = hidden.shape
    width = part * n * 2
    heads, half, size = states.shape[1:]
    channels = heads * half
    cols, maps = channels // n, input_proj.shape[1]
    aligned = all(v % LANES == 0 for v in (part, cols, maps, width, size, block_decay.shape[1]))
    if not (
        n & (n - 1) == 0
        and lax.axis_size("tp") == 2
        and states.shape[0] == 1
        and seqs == n
        and aligned
    ):
        return general(*args)
    f32, bf16 = jnp.float32, jnp.bfloat16
    (x,) = call(hold, [((seqs, part), bf16)], [hidden.T])
    (pair,) = call(stack, [((seqs, 2 * part), bf16)], [x, beside(x)])
    pieces = across([pair] * n)
    whole, step_pre, *sends = call(
        functools.partial(project, n),
        [((seqs, width), bf16), ((1, heads), f32)] + [((1, 2 * cols + 2 * maps), f32)] * n,
        pieces
        + [
            mixer_gain.reshape(1, width),
            gate_proj.transpose(1, 2, 0).reshape(cols, width),
            inner_proj.transpose(1, 2, 0).reshape(cols, width),
            input_proj,
            output_proj,
            step_proj.T,
        ],
    )
    pieces = across(sends)
    sends = call(
        functools.partial(mixer, n),
        [((1, cols + LANES), f32)] * n,
        [lengths]
        + pieces
        + [
            step_pre,
            step_bias.reshape(1, heads),
            decay_log.reshape(1, heads),
            skip_gain.reshape(1, heads),
            taps_inner.reshape(-1, channels),
            taps_input,
            taps_output,
            recent_inner.reshape(-1, channels),
            recent_input[0],
            recent_output[0],
            states.reshape(channels, size),
            block_inner.transpose(0, 2, 3, 1).reshape(channels, -1),
            block_input[0],
            block_decay[0].T,
            norm_gain.reshape(1, channels),
        ],
        scratch=[((1, channels), f32)] * 2 + [((1, n * maps), f32)] * 2 + [((1, channels), f32)],
        scalars=(0,),
    )
    pieces = across(sends)
    (mixed,) = call(
        functools.partial(out_project, n),
        [((seqs, width + LANES), f32)],
        pieces + [mixer_out.reshape(cols, width)],
        scratch=[((seqs, cols + LANES), f32)],
    )
    mixed, squares = call(
        add_pair,
        [((seqs, width), bf16), ((seqs, LANES), f32)],
        [mixed, beside(mixed)],
    )
    pieces = across([mixed] * n)
    mid, keep, send = call(
        functools.partial(channel_mix, n, 2 * channels),
        [((seqs, part), f32)] + [((seqs, width // 2), f32)] * 2,
        pieces
        + [squares, whole, channel_gain.reshape(1, width), expand_gate.T, expand_value.T, reduce_proj],
        scratch=[((seqs, width), f32)],
    )
    sends = call(
        split_pair,
        [((seqs, part), f32)] * n,
        [keep, beside(send)],
        scratch=[((seqs, width // 2), f32)],
    )
    pieces = across(sends)
    (out,) = call(functools.partial(finish, n), [((seqs, part), bf16)], pieces + [mid])
    return out.T


def solution(mesh):
    return jax.shard_map(
        layer,
        mesh=mesh,
        in_specs=(
            P(("kv", "tp"), "dp"),
            P(),
            P(None, "kv", "tp"),
            P(None, "kv", "tp"),
            P(None, "kv"),
            P(None, "kv"),
            P(),
            P(),
            P(),
            P(),
            P(None, None, "tp"),
            P(),
            P(),
            P(("dp", "kv"), None, None, "tp"),
            P(("dp", "kv"), None, None),
            P(("dp", "kv"), None, None),
            P(("dp", "kv"), None, "tp", None),
            P(("dp", "kv"), None, None, "tp"),
            P(("dp", "kv"), None, None),
            P(("dp", "kv"), None, None),
            P(("dp", "kv")),
            P(None, "tp"),
            P("kv", "tp", None),
            P(),
            P(None, ("kv", "tp")),
            P(None, ("kv", "tp")),
            P(("kv", "tp"), None),
        ),
        out_specs=P(("kv", "tp"), "dp"),
        check_vma=False,
    )
```

```python
import functools

import jax
import jax.numpy as jnp
from jax import lax
from jax.experimental import pallas as pl
from jax.experimental.pallas import tpu as pltpu
from jax.sharding import PartitionSpec as P


MIXER_HEADS = 64
HEAD_DIM = 64
GROUPS = 8
STATE = 128
OPEN_BLOCK_SPAN = 128


epsilon = 1e-05


def short_conv(recent, newest, taps):
    window = jnp.concatenate(
        [recent.astype(jnp.float32), newest.astype(jnp.float32)[:, None]], axis=1
    )
    return jax.nn.silu(jnp.sum(window * taps[None], axis=1))


def general(
    hidden,
    mixer_gain,
    gate_proj,
    inner_proj,
    input_proj,
    output_proj,
    step_proj,
    step_bias,
    decay_log,
    skip_gain,
    taps_inner,
    taps_input,
    taps_output,
    recent_inner,
    recent_input,
    recent_output,
    states,
    block_inner,
    block_input,
    block_decay,
    lengths,
    norm_gain,
    mixer_out,
    channel_gain,
    expand_gate,
    expand_value,
    reduce_proj,
):
    rows_own = hidden.shape[0]
    seq_all = hidden.shape[1]
    seq_dev = states.shape[0]
    half_dim = states.shape[2]
    width = rows_own * lax.axis_size("kv") * lax.axis_size("tp")
    offset = (lax.axis_index("kv") * lax.axis_size("tp") + lax.axis_index("tp")) * rows_own
    own_start = lax.axis_index("kv") * seq_dev
    whole_rows = lax.all_gather(hidden, ("kv", "tp"), axis=0, tiled=True)
    whole_f = whole_rows.astype(jnp.float32)
    rms_in = lax.rsqrt(jnp.mean(whole_f * whole_f, axis=0) + epsilon)
    normed_in = (whole_f * mixer_gain[:, None]).astype(jnp.bfloat16)
    gate_part = (
        rms_in[:, None, None]
        * jnp.einsum("ds,dhp->shp", normed_in, gate_proj, preferred_element_type=jnp.float32)
    ).astype(jnp.bfloat16)
    inner_part = (
        rms_in[:, None, None]
        * jnp.einsum("ds,dhp->shp", normed_in, inner_proj, preferred_element_type=jnp.float32)
    ).astype(jnp.bfloat16)
    input_part = (
        rms_in[:, None]
        * jnp.einsum("ds,dk->sk", normed_in, input_proj, preferred_element_type=jnp.float32)
    ).astype(jnp.bfloat16)
    output_part = (
        rms_in[:, None]
        * jnp.einsum("ds,dk->sk", normed_in, output_proj, preferred_element_type=jnp.float32)
    ).astype(jnp.bfloat16)
    own_cols = lax.dynamic_slice_in_dim(normed_in, own_start, seq_dev, 1)
    own_rms = lax.dynamic_slice_in_dim(rms_in, own_start, seq_dev, 0)
    step_pre = (
        own_rms[:, None]
        * jnp.einsum("ds,dh->sh", own_cols, step_proj, preferred_element_type=jnp.float32)
    ).astype(jnp.bfloat16)
    gate_pre, inner_pre, input_pre, output_pre = (
        lax.all_to_all(gate_part, "kv", split_axis=0, concat_axis=1, tiled=True),
        lax.all_to_all(inner_part, "kv", split_axis=0, concat_axis=1, tiled=True),
        lax.all_to_all(input_part, "kv", split_axis=0, concat_axis=1, tiled=True),
        lax.all_to_all(output_part, "kv", split_axis=0, concat_axis=1, tiled=True),
    )
    conv_inner = short_conv(recent_inner, inner_pre, taps_inner)
    conv_input = short_conv(recent_input, input_pre, taps_input)
    conv_output = short_conv(recent_output, output_pre, taps_output).astype(jnp.bfloat16)
    step = jax.nn.softplus(step_pre.astype(jnp.float32) + step_bias[None, :])
    new_decay = -jnp.exp(decay_log)[None, :] * step
    per_group = MIXER_HEADS // GROUPS
    live = (jnp.arange(OPEN_BLOCK_SPAN, dtype=jnp.int32)[None, :] < lengths[:, None]).astype(
        jnp.float32
    )
    masked = block_decay * live[:, :, None]
    cached = jnp.sum(masked, axis=1)
    tail = new_decay[:, None, :] + cached[:, None, :] - jnp.cumsum(masked, axis=1)
    total = new_decay + cached
    readout = conv_output.reshape(seq_dev, GROUPS, STATE)
    score = jnp.einsum(
        "sgn,sjgn->sgj",
        readout,
        block_input.reshape(seq_dev, OPEN_BLOCK_SPAN, GROUPS, STATE),
        preferred_element_type=jnp.float32,
    )
    score_heads = jnp.repeat(score, per_group, axis=1)
    weight = (live[:, None, :] * jnp.exp(jnp.swapaxes(tail, 1, 2)) * score_heads).astype(
        jnp.bfloat16
    )
    from_block = jnp.einsum(
        "shj,sjhp->shp", weight, block_inner, preferred_element_type=jnp.float32
    )
    readout_f = readout.astype(jnp.float32)
    grouped = states.reshape(seq_dev, GROUPS, per_group, half_dim, STATE)
    from_state = jnp.einsum(
        "sgn,sgrpn->sgrp", readout_f, grouped, precision=lax.Precision.HIGHEST
    ).reshape(seq_dev, MIXER_HEADS, half_dim)
    own_score = jnp.repeat(
        jnp.sum(readout_f * conv_input.reshape(seq_dev, GROUPS, STATE), axis=-1), per_group, axis=1
    )
    mix = (
        from_block
        + jnp.exp(total)[:, :, None] * from_state
        + (own_score * step)[:, :, None] * conv_inner
        + skip_gain[None, :, None] * conv_inner
    )
    gated_raw = mix * jax.nn.silu(gate_pre.astype(jnp.float32))
    part_squares = jnp.sum(gated_raw * gated_raw, axis=(1, 2))
    gated = (gated_raw * norm_gain[None]).astype(jnp.bfloat16)
    placed = lax.dynamic_update_slice_in_dim(
        jnp.zeros((seq_all,), jnp.float32), part_squares, own_start, 0
    )
    gate_squares = lax.psum(placed, ("kv", "tp"))
    rms_gate = lax.rsqrt(gate_squares / (MIXER_HEADS * HEAD_DIM) + epsilon)
    by_head = lax.all_to_all(gated, "kv", split_axis=1, concat_axis=0, tiled=True)
    columns = mixer_out
    mixed_full = rms_gate[None, :] * lax.psum(
        jnp.einsum("hpd,shp->ds", columns, by_head, preferred_element_type=jnp.float32),
        ("kv", "tp"),
    )
    mid_full = (whole_f + mixed_full).astype(jnp.bfloat16)
    mid = lax.dynamic_slice_in_dim(mid_full, offset, rows_own, 0)
    full_f = mid_full.astype(jnp.float32)
    mid_squares = jnp.sum(full_f * full_f, axis=0)
    normed_full = (full_f * channel_gain[:, None]).astype(jnp.bfloat16)
    gate_sum = jnp.einsum("ds,df->sf", normed_full, expand_gate, preferred_element_type=jnp.float32)
    value_sum = jnp.einsum(
        "ds,df->sf", normed_full, expand_value, preferred_element_type=jnp.float32
    )
    rms_mid = lax.rsqrt(mid_squares / width + epsilon)
    act = (jax.nn.silu(rms_mid[:, None] * gate_sum) * (rms_mid[:, None] * value_sum)).astype(
        jnp.bfloat16
    )
    columns = reduce_proj
    channel = lax.psum_scatter(
        jnp.einsum("fd,sf->ds", columns, act, preferred_element_type=jnp.float32),
        ("kv", "tp"),
        scatter_dimension=0,
        tiled=True,
    )
    return (mid.astype(jnp.float32) + channel).astype(jnp.bfloat16)


NT = (((1,), (1,)), ((), ()))
NN = (((1,), (0,)), ((), ()))
LANES = 128


def dot(a, b, dims, precision=None):
    return lax.dot_general(a, b, dims, precision=precision, preferred_element_type=jnp.float32)


def silu(v):
    return v / (1.0 + jnp.exp(-v))


def tree(values):
    values = list(values)
    while len(values) > 1:
        values = [a + b for a, b in zip(values[::2], values[1::2])]
    return values[0]


def call(body, outs, args, scratch=(), scalars=(), space=pltpu.VMEM):
    args = [
        a if i in scalars else pltpu.with_memory_space_constraint(a, pltpu.VMEM)
        for i, a in enumerate(args)
    ]
    return pl.pallas_call(
        body,
        out_shape=[space(s, d) for s, d in outs],
        in_specs=[
            pl.BlockSpec(memory_space=pltpu.SMEM if i in scalars else pltpu.VMEM)
            for i in range(len(args))
        ],
        out_specs=[pl.BlockSpec(memory_space=pltpu.VMEM) for _ in outs],
        scratch_shapes=[pltpu.VMEM(s, d) for s, d in scratch],
        compiler_params=pltpu.CompilerParams(vmem_limit_bytes=8 << 20),
        cost_estimate=pl.CostEstimate(flops=20_000_000_000, bytes_accessed=0, transcendentals=0),
    )(*args)


def lane(start, size):
    return pl.ds(pl.multiple_of(start, LANES), size)


def hold(a, out):
    out[...] = a[...]


def stack(a, b, out):
    part = a.shape[1]
    out[:, :part] = a[...]
    out[:, part:] = b[...]


def project(n, *refs):
    pieces, refs = refs[:n], refs[n:]
    mixer_gain, gate_w, inner_w, input_w, output_w, step_w = refs[:6]
    x_out, step_out = refs[6:8]
    sends = refs[8:]
    kv, tp = lax.axis_index("kv"), lax.axis_index("tp")
    width = x_out.shape[1]
    part = pieces[0].shape[1] // 2
    for k, ref in enumerate(pieces):
        base = (kv ^ k) * (2 * part)
        first = tp if k == 0 else 1 - tp
        x_out[:, lane(base + first * part, part)] = ref[:, :part]
        x_out[:, lane(base + (1 - first) * part, part)] = ref[:, part:]
    x = x_out[...].astype(jnp.float32)
    rms = lax.rsqrt(jnp.sum(x * x, axis=1, keepdims=True) / width + epsilon)
    normed = (x * mixer_gain[...]).astype(jnp.bfloat16)
    at = 0
    for weight, dims in ((gate_w, NT), (inner_w, NT), (input_w, NN), (output_w, NN)):
        value = rms * dot(normed, weight[...], dims)
        value = value.astype(jnp.bfloat16).astype(jnp.float32)
        row = lax.broadcasted_iota(jnp.int32, value.shape, 0)
        for k, ref in enumerate(sends):
            picked = jnp.sum(jnp.where(row == (kv ^ k), value, 0.0), axis=0, keepdims=True)
            ref[:, at : at + value.shape[1]] = picked
        at += value.shape[1]
    steps = (rms * dot(normed, step_w[...], NT)).astype(jnp.bfloat16).astype(jnp.float32)
    row = lax.broadcasted_iota(jnp.int32, steps.shape, 0)
    step_out[...] = jnp.sum(jnp.where(row == kv, steps, 0.0), axis=0, keepdims=True)


def mixer(n, length, *refs):
    pieces, refs = refs[:n], refs[n:]
    step_pre, step_bias, decay_log, skip_gain = refs[:4]
    taps_inner, taps_input, taps_output = refs[4:7]
    recent_inner, recent_input, recent_output = refs[7:10]
    states, block_inner, block_input, block_decay, norm_gain = refs[10:15]
    sends, (gate_row, inner_row, input_row, output_row, gated_row) = refs[15:-5], refs[-5:]
    kv = lax.axis_index("kv")
    heads, span = block_decay.shape
    channels = gate_row.shape[1]
    half = channels // heads
    size = states.shape[1]
    groups = block_input.shape[1] // size
    per_group = heads // groups
    chunk = per_group * half
    cols, maps = channels // n, input_row.shape[1] // n
    for k, ref in enumerate(pieces):
        src = kv ^ k
        gate_row[:, lane(src * cols, cols)] = ref[:, :cols]
        inner_row[:, lane(src * cols, cols)] = ref[:, cols : 2 * cols]
        input_row[:, lane(src * maps, maps)] = ref[:, 2 * cols : 2 * cols + maps]
        output_row[:, lane(src * maps, maps)] = ref[:, 2 * cols + maps :]

    def conv(recent, newest, taps):
        weights = taps[...]
        past = jnp.sum(recent[...].astype(jnp.float32) * weights[:-1], axis=0, keepdims=True)
        return silu(past + weights[-1:] * newest)

    conv_output = conv(recent_output, output_row[...], taps_output).astype(jnp.bfloat16)
    conv_input = conv(recent_input, input_row[...], taps_input)
    conv_inner = conv(recent_inner, inner_row[...], taps_inner)
    readout = conv_output.astype(jnp.float32)

    eye = lax.broadcasted_iota(jnp.int32, (heads, heads), 0) == lax.broadcasted_iota(
        jnp.int32, (heads, heads), 1
    )

    def column(row):
        return jnp.sum(jnp.where(eye, row, 0.0), axis=1, keepdims=True)

    pre = step_pre[...] + step_bias[...]
    step_row = jnp.maximum(pre, 0.0) + jnp.log1p(jnp.exp(-jnp.abs(pre)))
    step = column(step_row)
    new_decay = column(-jnp.exp(decay_log[...]) * step_row)
    skip = column(skip_gain[...])

    live = (lax.broadcasted_iota(jnp.int32, (1, span), 1) < length[0]).astype(jnp.float32)
    masked = block_decay[...] * live
    later = (
        lax.broadcasted_iota(jnp.int32, (span, span), 0)
        > lax.broadcasted_iota(jnp.int32, (span, span), 1)
    ).astype(jnp.float32)
    suffix = dot(masked, later, NN, lax.Precision.HIGHEST)
    grown = jnp.exp(new_decay + jnp.sum(masked, axis=1, keepdims=True))
    decayed = live * jnp.exp(new_decay + suffix)

    wide = (groups, groups * size)
    diagonal = lax.broadcasted_iota(jnp.int32, wide, 1) // size == lax.broadcasted_iota(
        jnp.int32, wide, 0
    )
    spread = jnp.where(diagonal, readout, 0.0)
    score = dot(spread.astype(jnp.bfloat16), block_input[...], NT)
    own_score = jnp.sum(spread * conv_input, axis=1, keepdims=True)

    narrow = (per_group, chunk)
    mine = lax.broadcasted_iota(jnp.int32, narrow, 1) // half == lax.broadcasted_iota(
        jnp.int32, narrow, 0
    )
    squares = jnp.zeros((1, chunk), jnp.float32)
    for g in range(groups):
        head = slice(g * per_group, (g + 1) * per_group)
        rows = slice(g * chunk, (g + 1) * chunk)
        weight = (decayed[head] * score[g : g + 1]).astype(jnp.bfloat16)
        from_block = dot(weight, block_inner[rows, :], NT)
        state = states[rows, :]
        high = state.astype(jnp.bfloat16)
        low = (state - high.astype(jnp.float32)).astype(jnp.bfloat16)
        out_map = jnp.broadcast_to(
            readout[:, g * size : (g + 1) * size], (per_group, size)
        ).astype(jnp.bfloat16)
        from_state = dot(out_map, high, NT) + dot(out_map, low, NT)
        direct = own_score[g : g + 1] * step[head] + skip[head]
        both = from_block + grown[head] * from_state + direct * conv_inner[:, rows]
        mix = jnp.sum(jnp.where(mine, both, 0.0), axis=0, keepdims=True)
        raw = mix * silu(gate_row[:, rows])
        squares = squares + raw * raw
        gated_row[:, rows] = (raw * norm_gain[:, rows]).astype(jnp.bfloat16).astype(jnp.float32)
    square = jnp.sum(squares, axis=1, keepdims=True)
    for k, ref in enumerate(sends):
        ref[:, :cols] = gated_row[:, lane((kv ^ k) * cols, cols)]
        ref[:, cols:] = jnp.broadcast_to(square, (1, LANES))


def out_project(n, *refs):
    pieces, (mixer_out, out, rows) = refs[:n], refs[n:]
    kv = lax.axis_index("kv")
    cols, width = mixer_out.shape
    for k, ref in enumerate(pieces):
        rows[pl.ds(kv ^ k, 1), :] = ref[...]
    out[:, :width] = dot(rows[:, :cols].astype(jnp.bfloat16), mixer_out[...], NN)
    out[:, width:] = rows[:, cols:]


def add_pair(a, b, out, squares):
    width = out.shape[1]
    out[...] = (a[:, :width] + b[:, :width]).astype(jnp.bfloat16)
    squares[...] = a[:, width:] + b[:, width:]


def channel_mix(n, channels, *refs):
    pieces, (squares, x, gain, gate_w, value_w, reduce_w) = refs[:n], refs[n : n + 6]
    mid_out, keep, send, moved = refs[n + 6 :]
    kv, tp = lax.axis_index("kv"), lax.axis_index("tp")
    width = x.shape[1]
    part = mid_out.shape[1]
    whole = tree(ref[...].astype(jnp.float32) for ref in pieces)
    rms_gate = lax.rsqrt(squares[:, :1] / channels + epsilon)
    mid = (x[...].astype(jnp.float32) + rms_gate * whole).astype(jnp.bfloat16)
    mid = mid.astype(jnp.float32)
    rms = lax.rsqrt(jnp.sum(mid * mid, axis=1, keepdims=True) / width + epsilon)
    normed = (mid * gain[...]).astype(jnp.bfloat16)
    moved[...] = mid
    mid_out[...] = moved[:, lane((kv * 2 + tp) * part, part)]
    act = silu(rms * dot(normed, gate_w[...], NT)) * (rms * dot(normed, value_w[...], NT))
    moved[...] = dot(act.astype(jnp.bfloat16), reduce_w[...], NN)
    for k in range(n):
        at = slice(k * part, (k + 1) * part)
        side = tp if k == 0 else 1 - tp
        keep[:, at] = moved[:, lane((2 * (kv ^ k) + side) * part, part)]
        send[:, at] = moved[:, lane((2 * (kv ^ k) + 1 - side) * part, part)]


def split_pair(a, b, *outs):
    part = outs[0].shape[1]
    for k, ref in enumerate(outs):
        at = slice(k * part, (k + 1) * part)
        ref[...] = a[:, at] + b[:, at]


def finish(n, *refs):
    pieces, (mid, out) = refs[:n], refs[n:]
    out[...] = (mid[...] + tree(ref[...] for ref in pieces)).astype(jnp.bfloat16)


def across(values, cross=False):
    n = len(values)
    got = [values[0]] + [None] * (n - 1)
    for k in range(1, n):
        if cross:
            pairs = [(i, i ^ (2 * k + 1)) for i in range(2 * n)]
            got[k] = lax.ppermute(values[k], ("kv", "tp"), pairs)
        else:
            got[k] = lax.ppermute(values[k], "kv", [(i, i ^ k) for i in range(n)])
    return got


def beside(value):
    return lax.ppermute(value, "tp", [(0, 1), (1, 0)])


def layer(*args):
    (
        hidden, mixer_gain, gate_proj, inner_proj, input_proj, output_proj, step_proj, step_bias,
        decay_log, skip_gain, taps_inner, taps_input, taps_output, recent_inner, recent_input,
        recent_output, states, block_inner, block_input, block_decay, lengths, norm_gain, mixer_out,
        channel_gain, expand_gate, expand_value, reduce_proj,
    ) = args
    n = lax.axis_size("kv")
    part, seqs = hidden.shape
    width = part * n * 2
    heads, half, size = states.shape[1:]
    channels = heads * half
    cols, maps = channels // n, input_proj.shape[1]
    aligned = all(v % LANES == 0 for v in (part, cols, maps, width, size, block_decay.shape[1]))
    if not (
        n & (n - 1) == 0
        and lax.axis_size("tp") == 2
        and states.shape[0] == 1
        and seqs == n
        and aligned
    ):
        return general(*args)
    f32, bf16 = jnp.float32, jnp.bfloat16
    x = hidden.T
    other = beside(x)
    (x,) = call(hold, [((seqs, part), bf16)], [x])
    (pair,) = call(stack, [((seqs, 2 * part), bf16)], [x, other])
    pieces = across([pair] * n, cross=True)
    whole, step_pre, *sends = call(
        functools.partial(project, n),
        [((seqs, width), bf16), ((1, heads), f32)] + [((1, 2 * cols + 2 * maps), f32)] * n,
        pieces
        + [
            mixer_gain.reshape(1, width),
            gate_proj.transpose(1, 2, 0).reshape(cols, width),
            inner_proj.transpose(1, 2, 0).reshape(cols, width),
            input_proj,
            output_proj,
            step_proj.T,
        ],
    )
    pieces = across(sends)
    sends = call(
        functools.partial(mixer, n),
        [((1, cols + LANES), f32)] * n,
        [lengths]
        + pieces
        + [
            step_pre,
            step_bias.reshape(1, heads),
            decay_log.reshape(1, heads),
            skip_gain.reshape(1, heads),
            taps_inner.reshape(-1, channels),
            taps_input,
            taps_output,
            recent_inner.reshape(-1, channels),
            recent_input[0],
            recent_output[0],
            states.reshape(channels, size),
            block_inner.transpose(0, 2, 3, 1).reshape(channels, -1),
            block_input[0],
            block_decay[0].T,
            norm_gain.reshape(1, channels),
        ],
        scratch=[((1, channels), f32)] * 2 + [((1, n * maps), f32)] * 2 + [((1, channels), f32)],
        scalars=(0,),
    )
    pieces = across(sends)
    (mixed,) = call(
        functools.partial(out_project, n),
        [((seqs, width + LANES), f32)],
        pieces + [mixer_out.reshape(cols, width)],
        scratch=[((seqs, cols + LANES), f32)],
    )
    mixed, squares = call(
        add_pair,
        [((seqs, width), bf16), ((seqs, LANES), f32)],
        [mixed, beside(mixed)],
    )
    pieces = across([mixed] * n, cross=True)
    mid, keep, send = call(
        functools.partial(channel_mix, n, 2 * channels),
        [((seqs, part), f32)] + [((seqs, width // 2), f32)] * 2,
        pieces
        + [squares, whole, channel_gain.reshape(1, width), expand_gate.T, expand_value.T, reduce_proj],
        scratch=[((seqs, width), f32)],
    )
    sends = call(split_pair, [((seqs, part), f32)] * n, [keep, beside(send)])
    pieces = across(sends, cross=True)
    (out,) = call(
        functools.partial(finish, n),
        [((seqs, part), bf16)],
        pieces + [mid],
        space=jax.ShapeDtypeStruct,
    )
    return out.T


def solution(mesh):
    return jax.shard_map(
        layer,
        mesh=mesh,
        in_specs=(
            P(("kv", "tp"), "dp"),
            P(),
            P(None, "kv", "tp"),
            P(None, "kv", "tp"),
            P(None, "kv"),
            P(None, "kv"),
            P(),
            P(),
            P(),
            P(),
            P(None, None, "tp"),
            P(),
            P(),
            P(("dp", "kv"), None, None, "tp"),
            P(("dp", "kv"), None, None),
            P(("dp", "kv"), None, None),
            P(("dp", "kv"), None, "tp", None),
            P(("dp", "kv"), None, None, "tp"),
            P(("dp", "kv"), None, None),
            P(("dp", "kv"), None, None),
            P(("dp", "kv")),
            P(None, "tp"),
            P("kv", "tp", None),
            P(),
            P(None, ("kv", "tp")),
            P(None, ("kv", "tp")),
            P(("kv", "tp"), None),
        ),
        out_specs=P(("kv", "tp"), "dp"),
        check_vma=False,
    )
```

```python
import functools

import jax
import jax.numpy as jnp
from jax import lax
from jax.experimental import pallas as pl
from jax.experimental.pallas import tpu as pltpu
from jax.sharding import PartitionSpec as P


MIXER_HEADS = 64
HEAD_DIM = 64
GROUPS = 8
STATE = 128
OPEN_BLOCK_SPAN = 128


epsilon = 1e-05


def short_conv(recent, newest, taps):
    window = jnp.concatenate(
        [recent.astype(jnp.float32), newest.astype(jnp.float32)[:, None]], axis=1
    )
    return jax.nn.silu(jnp.sum(window * taps[None], axis=1))


def general(
    hidden,
    mixer_gain,
    gate_proj,
    inner_proj,
    input_proj,
    output_proj,
    step_proj,
    step_bias,
    decay_log,
    skip_gain,
    taps_inner,
    taps_input,
    taps_output,
    recent_inner,
    recent_input,
    recent_output,
    states,
    block_inner,
    block_input,
    block_decay,
    lengths,
    norm_gain,
    mixer_out,
    channel_gain,
    expand_gate,
    expand_value,
    reduce_proj,
):
    rows_own = hidden.shape[0]
    seq_all = hidden.shape[1]
    seq_dev = states.shape[0]
    half_dim = states.shape[2]
    width = rows_own * lax.axis_size("kv") * lax.axis_size("tp")
    offset = (lax.axis_index("kv") * lax.axis_size("tp") + lax.axis_index("tp")) * rows_own
    own_start = lax.axis_index("kv") * seq_dev
    whole_rows = lax.all_gather(hidden, ("kv", "tp"), axis=0, tiled=True)
    whole_f = whole_rows.astype(jnp.float32)
    rms_in = lax.rsqrt(jnp.mean(whole_f * whole_f, axis=0) + epsilon)
    normed_in = (whole_f * mixer_gain[:, None]).astype(jnp.bfloat16)
    gate_part = (
        rms_in[:, None, None]
        * jnp.einsum("ds,dhp->shp", normed_in, gate_proj, preferred_element_type=jnp.float32)
    ).astype(jnp.bfloat16)
    inner_part = (
        rms_in[:, None, None]
        * jnp.einsum("ds,dhp->shp", normed_in, inner_proj, preferred_element_type=jnp.float32)
    ).astype(jnp.bfloat16)
    input_part = (
        rms_in[:, None]
        * jnp.einsum("ds,dk->sk", normed_in, input_proj, preferred_element_type=jnp.float32)
    ).astype(jnp.bfloat16)
    output_part = (
        rms_in[:, None]
        * jnp.einsum("ds,dk->sk", normed_in, output_proj, preferred_element_type=jnp.float32)
    ).astype(jnp.bfloat16)
    own_cols = lax.dynamic_slice_in_dim(normed_in, own_start, seq_dev, 1)
    own_rms = lax.dynamic_slice_in_dim(rms_in, own_start, seq_dev, 0)
    step_pre = (
        own_rms[:, None]
        * jnp.einsum("ds,dh->sh", own_cols, step_proj, preferred_element_type=jnp.float32)
    ).astype(jnp.bfloat16)
    gate_pre, inner_pre, input_pre, output_pre = (
        lax.all_to_all(gate_part, "kv", split_axis=0, concat_axis=1, tiled=True),
        lax.all_to_all(inner_part, "kv", split_axis=0, concat_axis=1, tiled=True),
        lax.all_to_all(input_part, "kv", split_axis=0, concat_axis=1, tiled=True),
        lax.all_to_all(output_part, "kv", split_axis=0, concat_axis=1, tiled=True),
    )
    conv_inner = short_conv(recent_inner, inner_pre, taps_inner)
    conv_input = short_conv(recent_input, input_pre, taps_input)
    conv_output = short_conv(recent_output, output_pre, taps_output).astype(jnp.bfloat16)
    step = jax.nn.softplus(step_pre.astype(jnp.float32) + step_bias[None, :])
    new_decay = -jnp.exp(decay_log)[None, :] * step
    per_group = MIXER_HEADS // GROUPS
    live = (jnp.arange(OPEN_BLOCK_SPAN, dtype=jnp.int32)[None, :] < lengths[:, None]).astype(
        jnp.float32
    )
    masked = block_decay * live[:, :, None]
    cached = jnp.sum(masked, axis=1)
    tail = new_decay[:, None, :] + cached[:, None, :] - jnp.cumsum(masked, axis=1)
    total = new_decay + cached
    readout = conv_output.reshape(seq_dev, GROUPS, STATE)
    score = jnp.einsum(
        "sgn,sjgn->sgj",
        readout,
        block_input.reshape(seq_dev, OPEN_BLOCK_SPAN, GROUPS, STATE),
        preferred_element_type=jnp.float32,
    )
    score_heads = jnp.repeat(score, per_group, axis=1)
    weight = (live[:, None, :] * jnp.exp(jnp.swapaxes(tail, 1, 2)) * score_heads).astype(
        jnp.bfloat16
    )
    from_block = jnp.einsum(
        "shj,sjhp->shp", weight, block_inner, preferred_element_type=jnp.float32
    )
    readout_f = readout.astype(jnp.float32)
    grouped = states.reshape(seq_dev, GROUPS, per_group, half_dim, STATE)
    from_state = jnp.einsum(
        "sgn,sgrpn->sgrp", readout_f, grouped, precision=lax.Precision.HIGHEST
    ).reshape(seq_dev, MIXER_HEADS, half_dim)
    own_score = jnp.repeat(
        jnp.sum(readout_f * conv_input.reshape(seq_dev, GROUPS, STATE), axis=-1), per_group, axis=1
    )
    mix = (
        from_block
        + jnp.exp(total)[:, :, None] * from_state
        + (own_score * step)[:, :, None] * conv_inner
        + skip_gain[None, :, None] * conv_inner
    )
    gated_raw = mix * jax.nn.silu(gate_pre.astype(jnp.float32))
    part_squares = jnp.sum(gated_raw * gated_raw, axis=(1, 2))
    gated = (gated_raw * norm_gain[None]).astype(jnp.bfloat16)
    placed = lax.dynamic_update_slice_in_dim(
        jnp.zeros((seq_all,), jnp.float32), part_squares, own_start, 0
    )
    gate_squares = lax.psum(placed, ("kv", "tp"))
    rms_gate = lax.rsqrt(gate_squares / (MIXER_HEADS * HEAD_DIM) + epsilon)
    by_head = lax.all_to_all(gated, "kv", split_axis=1, concat_axis=0, tiled=True)
    columns = mixer_out
    mixed_full = rms_gate[None, :] * lax.psum(
        jnp.einsum("hpd,shp->ds", columns, by_head, preferred_element_type=jnp.float32),
        ("kv", "tp"),
    )
    mid_full = (whole_f + mixed_full).astype(jnp.bfloat16)
    mid = lax.dynamic_slice_in_dim(mid_full, offset, rows_own, 0)
    full_f = mid_full.astype(jnp.float32)
    mid_squares = jnp.sum(full_f * full_f, axis=0)
    normed_full = (full_f * channel_gain[:, None]).astype(jnp.bfloat16)
    gate_sum = jnp.einsum("ds,df->sf", normed_full, expand_gate, preferred_element_type=jnp.float32)
    value_sum = jnp.einsum(
        "ds,df->sf", normed_full, expand_value, preferred_element_type=jnp.float32
    )
    rms_mid = lax.rsqrt(mid_squares / width + epsilon)
    act = (jax.nn.silu(rms_mid[:, None] * gate_sum) * (rms_mid[:, None] * value_sum)).astype(
        jnp.bfloat16
    )
    columns = reduce_proj
    channel = lax.psum_scatter(
        jnp.einsum("fd,sf->ds", columns, act, preferred_element_type=jnp.float32),
        ("kv", "tp"),
        scatter_dimension=0,
        tiled=True,
    )
    return (mid.astype(jnp.float32) + channel).astype(jnp.bfloat16)


NT = (((1,), (1,)), ((), ()))
NN = (((1,), (0,)), ((), ()))
LANES = 128


def dot(a, b, dims, precision=None):
    return lax.dot_general(a, b, dims, precision=precision, preferred_element_type=jnp.float32)


def silu(v):
    return v / (1.0 + jnp.exp(-v))


def tree(values):
    values = list(values)
    while len(values) > 1:
        values = [a + b for a, b in zip(values[::2], values[1::2])]
    return values[0]


def call(body, outs, args, scratch=(), scalars=(), space=pltpu.VMEM):
    args = [
        a if i in scalars else pltpu.with_memory_space_constraint(a, pltpu.VMEM)
        for i, a in enumerate(args)
    ]
    return pl.pallas_call(
        body,
        out_shape=[space(s, d) for s, d in outs],
        in_specs=[
            pl.BlockSpec(memory_space=pltpu.SMEM if i in scalars else pltpu.VMEM)
            for i in range(len(args))
        ],
        out_specs=[pl.BlockSpec(memory_space=pltpu.VMEM) for _ in outs],
        scratch_shapes=[pltpu.VMEM(s, d) for s, d in scratch],
        compiler_params=pltpu.CompilerParams(vmem_limit_bytes=8 << 20),
        cost_estimate=pl.CostEstimate(flops=20_000_000_000, bytes_accessed=0, transcendentals=0),
    )(*args)


def lane(start, size):
    return pl.ds(pl.multiple_of(start, LANES), size)


def hold(a, out):
    out[...] = a[...]


def stack(a, b, out):
    part = a.shape[1]
    out[:, :part] = a[...]
    out[:, part:] = b[...]


def project(n, *refs):
    pieces, refs = refs[:n], refs[n:]
    mixer_gain, gate_w, inner_w, input_w, output_w, step_w = refs[:6]
    x_out, step_out = refs[6:8]
    sends = refs[8:]
    kv, tp = lax.axis_index("kv"), lax.axis_index("tp")
    width = x_out.shape[1]
    part = pieces[0].shape[1] // 2
    for k, ref in enumerate(pieces):
        base = (kv ^ k) * (2 * part)
        first = tp if k == 0 else 1 - tp
        x_out[:, lane(base + first * part, part)] = ref[:, :part]
        x_out[:, lane(base + (1 - first) * part, part)] = ref[:, part:]
    x = x_out[...].astype(jnp.float32)
    rms = lax.rsqrt(jnp.sum(x * x, axis=1, keepdims=True) / width + epsilon)
    normed = (x * mixer_gain[...]).astype(jnp.bfloat16)
    at = 0
    for weight, dims in ((gate_w, NT), (inner_w, NT), (input_w, NN), (output_w, NN)):
        value = rms * dot(normed, weight[...], dims)
        value = value.astype(jnp.bfloat16).astype(jnp.float32)
        row = lax.broadcasted_iota(jnp.int32, value.shape, 0)
        for k, ref in enumerate(sends):
            picked = jnp.sum(jnp.where(row == (kv ^ k), value, 0.0), axis=0, keepdims=True)
            ref[:, at : at + value.shape[1]] = picked
        at += value.shape[1]
    steps = (rms * dot(normed, step_w[...], NT)).astype(jnp.bfloat16).astype(jnp.float32)
    row = lax.broadcasted_iota(jnp.int32, steps.shape, 0)
    step_out[...] = jnp.sum(jnp.where(row == kv, steps, 0.0), axis=0, keepdims=True)


def mixer(n, length, *refs):
    pieces, refs = refs[:n], refs[n:]
    step_pre, step_bias, decay_log, skip_gain = refs[:4]
    taps_inner, taps_input, taps_output = refs[4:7]
    recent_inner, recent_input, recent_output = refs[7:10]
    states, block_inner, block_input, block_decay, norm_gain = refs[10:15]
    sends, (gate_row, inner_row, input_row, output_row, gated_row) = refs[15:-5], refs[-5:]
    kv = lax.axis_index("kv")
    heads, span = block_decay.shape
    channels = gate_row.shape[1]
    half = channels // heads
    size = states.shape[1]
    groups = block_input.shape[1] // size
    per_group = heads // groups
    chunk = per_group * half
    cols, maps = channels // n, input_row.shape[1] // n
    for k, ref in enumerate(pieces):
        src = kv ^ k
        gate_row[:, lane(src * cols, cols)] = ref[:, :cols]
        inner_row[:, lane(src * cols, cols)] = ref[:, cols : 2 * cols]
        input_row[:, lane(src * maps, maps)] = ref[:, 2 * cols : 2 * cols + maps]
        output_row[:, lane(src * maps, maps)] = ref[:, 2 * cols + maps :]

    def conv(recent, newest, taps):
        weights = taps[...]
        past = jnp.sum(recent[...].astype(jnp.float32) * weights[:-1], axis=0, keepdims=True)
        return silu(past + weights[-1:] * newest)

    conv_output = conv(recent_output, output_row[...], taps_output).astype(jnp.bfloat16)
    conv_input = conv(recent_input, input_row[...], taps_input)
    conv_inner = conv(recent_inner, inner_row[...], taps_inner)
    readout = conv_output.astype(jnp.float32)

    eye = lax.broadcasted_iota(jnp.int32, (heads, heads), 0) == lax.broadcasted_iota(
        jnp.int32, (heads, heads), 1
    )

    def column(row):
        return jnp.sum(jnp.where(eye, row, 0.0), axis=1, keepdims=True)

    pre = step_pre[...] + step_bias[...]
    step_row = jnp.maximum(pre, 0.0) + jnp.log1p(jnp.exp(-jnp.abs(pre)))
    step = column(step_row)
    new_decay = column(-jnp.exp(decay_log[...]) * step_row)
    skip = column(skip_gain[...])

    live = (lax.broadcasted_iota(jnp.int32, (1, span), 1) < length[0]).astype(jnp.float32)
    masked = block_decay[...] * live
    later = (
        lax.broadcasted_iota(jnp.int32, (span, span), 0)
        > lax.broadcasted_iota(jnp.int32, (span, span), 1)
    ).astype(jnp.float32)
    suffix = dot(masked, later, NN, lax.Precision.HIGHEST)
    grown = jnp.exp(new_decay + jnp.sum(masked, axis=1, keepdims=True))
    decayed = live * jnp.exp(new_decay + suffix)

    wide = (groups, groups * size)
    diagonal = lax.broadcasted_iota(jnp.int32, wide, 1) // size == lax.broadcasted_iota(
        jnp.int32, wide, 0
    )
    spread = jnp.where(diagonal, readout, 0.0)
    score = dot(spread.astype(jnp.bfloat16), block_input[...], NT)
    own_score = jnp.sum(spread * conv_input, axis=1, keepdims=True)

    narrow = (per_group, chunk)
    mine = lax.broadcasted_iota(jnp.int32, narrow, 1) // half == lax.broadcasted_iota(
        jnp.int32, narrow, 0
    )
    squares = jnp.zeros((1, chunk), jnp.float32)
    for g in range(groups):
        head = slice(g * per_group, (g + 1) * per_group)
        rows = slice(g * chunk, (g + 1) * chunk)
        weight = (decayed[head] * score[g : g + 1]).astype(jnp.bfloat16)
        from_block = dot(weight, block_inner[rows, :], NT)
        state = states[rows, :]
        high = state.astype(jnp.bfloat16)
        low = (state - high.astype(jnp.float32)).astype(jnp.bfloat16)
        out_map = jnp.broadcast_to(
            readout[:, g * size : (g + 1) * size], (per_group, size)
        ).astype(jnp.bfloat16)
        from_state = dot(out_map, high, NT) + dot(out_map, low, NT)
        direct = own_score[g : g + 1] * step[head] + skip[head]
        both = from_block + grown[head] * from_state + direct * conv_inner[:, rows]
        mix = jnp.sum(jnp.where(mine, both, 0.0), axis=0, keepdims=True)
        raw = mix * silu(gate_row[:, rows])
        squares = squares + raw * raw
        gated_row[:, rows] = (raw * norm_gain[:, rows]).astype(jnp.bfloat16).astype(jnp.float32)
    square = jnp.sum(squares, axis=1, keepdims=True)
    for k, ref in enumerate(sends):
        ref[:, :cols] = gated_row[:, lane((kv ^ k) * cols, cols)]
        ref[:, cols:] = jnp.broadcast_to(square, (1, LANES))


def out_project(n, *refs):
    pieces, (mixer_out, out, rows) = refs[:n], refs[n:]
    kv = lax.axis_index("kv")
    cols, width = mixer_out.shape
    for k, ref in enumerate(pieces):
        rows[pl.ds(kv ^ k, 1), :] = ref[...]
    out[:, :width] = dot(rows[:, :cols].astype(jnp.bfloat16), mixer_out[...], NN)
    out[:, width:] = rows[:, cols:]


def add_pair(a, b, out, squares):
    width = out.shape[1]
    out[...] = (a[:, :width] + b[:, :width]).astype(jnp.bfloat16)
    squares[...] = a[:, width:] + b[:, width:]


def channel_mix(n, channels, *refs):
    pieces, (squares, x, gain, gate_w, value_w, reduce_w) = refs[:n], refs[n : n + 6]
    mid_out, keep, send, moved = refs[n + 6 :]
    kv, tp = lax.axis_index("kv"), lax.axis_index("tp")
    width = x.shape[1]
    part = mid_out.shape[1]
    whole = tree(ref[...].astype(jnp.float32) for ref in pieces)
    rms_gate = lax.rsqrt(squares[:, :1] / channels + epsilon)
    mid = (x[...].astype(jnp.float32) + rms_gate * whole).astype(jnp.bfloat16)
    mid = mid.astype(jnp.float32)
    rms = lax.rsqrt(jnp.sum(mid * mid, axis=1, keepdims=True) / width + epsilon)
    normed = (mid * gain[...]).astype(jnp.bfloat16)
    moved[...] = mid
    mid_out[...] = moved[:, lane((kv * 2 + tp) * part, part)]
    act = silu(rms * dot(normed, gate_w[...], NT)) * (rms * dot(normed, value_w[...], NT))
    moved[...] = dot(act.astype(jnp.bfloat16), reduce_w[...], NN)
    for k in range(n):
        at = slice(k * part, (k + 1) * part)
        side = tp if k == 0 else 1 - tp
        keep[:, at] = moved[:, lane((2 * (kv ^ k) + side) * part, part)]
        send[:, at] = moved[:, lane((2 * (kv ^ k) + 1 - side) * part, part)]


def split_pair(a, b, *outs):
    part = outs[0].shape[1]
    for k, ref in enumerate(outs):
        at = slice(k * part, (k + 1) * part)
        ref[...] = a[:, at] + b[:, at]


def finish(n, *refs):
    pieces, (mid, out) = refs[:n], refs[n:]
    out[...] = (mid[...] + tree(ref[...] for ref in pieces)).astype(jnp.bfloat16)


def across(values, first=1):
    n = len(values)
    got = list(values[:first])
    for k in range(first, n):
        pairs = [(i, i ^ (2 * k + 1)) for i in range(2 * n)]
        got.append(lax.ppermute(values[k], ("kv", "tp"), pairs))
    return got


def beside(value):
    return lax.ppermute(value, "tp", [(0, 1), (1, 0)])


def layer(*args):
    (
        hidden, mixer_gain, gate_proj, inner_proj, input_proj, output_proj, step_proj, step_bias,
        decay_log, skip_gain, taps_inner, taps_input, taps_output, recent_inner, recent_input,
        recent_output, states, block_inner, block_input, block_decay, lengths, norm_gain, mixer_out,
        channel_gain, expand_gate, expand_value, reduce_proj,
    ) = args
    n = lax.axis_size("kv")
    part, seqs = hidden.shape
    width = part * n * 2
    heads, half, size = states.shape[1:]
    channels = heads * half
    cols, maps = channels // n, input_proj.shape[1]
    aligned = all(v % LANES == 0 for v in (part, cols, maps, width, size, block_decay.shape[1]))
    if not (
        n & (n - 1) == 0
        and lax.axis_size("tp") == 2
        and states.shape[0] == 1
        and seqs == n
        and aligned
    ):
        return general(*args)
    f32, bf16 = jnp.float32, jnp.bfloat16
    x = hidden.T
    other = beside(x)
    (x,) = call(hold, [((seqs, part), bf16)], [x])
    (pair,) = call(stack, [((seqs, 2 * part), bf16)], [x, other])
    pieces = across([pair] * n)
    states, block_inner, taps_inner, recent_inner, norm_gain = (
        beside(v)
        for v in (states, block_inner, taps_inner, recent_inner, norm_gain)
    )
    whole, step_pre, *sends = call(
        functools.partial(project, n),
        [((seqs, width), bf16), ((1, heads), f32)] + [((1, 2 * cols + 2 * maps), f32)] * n,
        pieces
        + [
            mixer_gain.reshape(1, width),
            gate_proj.transpose(1, 2, 0).reshape(cols, width),
            inner_proj.transpose(1, 2, 0).reshape(cols, width),
            input_proj,
            output_proj,
            step_proj.T,
        ],
    )
    pieces = across(sends, first=0)
    sends = call(
        functools.partial(mixer, n),
        [((1, cols + LANES), f32)] * n,
        [lengths]
        + pieces
        + [
            step_pre,
            step_bias.reshape(1, heads),
            decay_log.reshape(1, heads),
            skip_gain.reshape(1, heads),
            taps_inner.reshape(-1, channels),
            taps_input,
            taps_output,
            recent_inner.reshape(-1, channels),
            recent_input[0],
            recent_output[0],
            states.reshape(channels, size),
            block_inner.transpose(0, 2, 3, 1).reshape(channels, -1),
            block_input[0],
            block_decay[0].T,
            norm_gain.reshape(1, channels),
        ],
        scratch=[((1, channels), f32)] * 2 + [((1, n * maps), f32)] * 2 + [((1, channels), f32)],
        scalars=(0,),
    )
    pieces = across(sends, first=0)
    (mixed,) = call(
        functools.partial(out_project, n),
        [((seqs, width + LANES), f32)],
        pieces + [mixer_out.reshape(cols, width)],
        scratch=[((seqs, cols + LANES), f32)],
    )
    mixed, squares = call(
        add_pair,
        [((seqs, width), bf16), ((seqs, LANES), f32)],
        [mixed, beside(mixed)],
    )
    pieces = across([mixed] * n)
    mid, keep, send = call(
        functools.partial(channel_mix, n, 2 * channels),
        [((seqs, part), f32)] + [((seqs, width // 2), f32)] * 2,
        pieces
        + [squares, whole, channel_gain.reshape(1, width), expand_gate.T, expand_value.T, reduce_proj],
        scratch=[((seqs, width), f32)],
    )
    sends = call(split_pair, [((seqs, part), f32)] * n, [keep, beside(send)])
    pieces = across(sends)
    (out,) = call(
        functools.partial(finish, n),
        [((seqs, part), bf16)],
        pieces + [mid],
        space=jax.ShapeDtypeStruct,
    )
    return out.T


def solution(mesh):
    return jax.shard_map(
        layer,
        mesh=mesh,
        in_specs=(
            P(("kv", "tp"), "dp"),
            P(),
            P(None, "kv", "tp"),
            P(None, "kv", "tp"),
            P(None, "kv"),
            P(None, "kv"),
            P(),
            P(),
            P(),
            P(),
            P(None, None, "tp"),
            P(),
            P(),
            P(("dp", "kv"), None, None, "tp"),
            P(("dp", "kv"), None, None),
            P(("dp", "kv"), None, None),
            P(("dp", "kv"), None, "tp", None),
            P(("dp", "kv"), None, None, "tp"),
            P(("dp", "kv"), None, None),
            P(("dp", "kv"), None, None),
            P(("dp", "kv")),
            P(None, "tp"),
            P("kv", "tp", None),
            P(),
            P(None, ("kv", "tp")),
            P(None, ("kv", "tp")),
            P(("kv", "tp"), None),
        ),
        out_specs=P(("kv", "tp"), "dp"),
        check_vma=False,
    )
```

```python
import functools

import jax
import jax.numpy as jnp
from jax import lax
from jax.experimental import pallas as pl
from jax.experimental.pallas import tpu as pltpu
from jax.sharding import PartitionSpec as P


MIXER_HEADS = 64
HEAD_DIM = 64
GROUPS = 8
STATE = 128
OPEN_BLOCK_SPAN = 128


epsilon = 1e-05


def short_conv(recent, newest, taps):
    window = jnp.concatenate(
        [recent.astype(jnp.float32), newest.astype(jnp.float32)[:, None]], axis=1
    )
    return jax.nn.silu(jnp.sum(window * taps[None], axis=1))


def general(
    hidden,
    mixer_gain,
    gate_proj,
    inner_proj,
    input_proj,
    output_proj,
    step_proj,
    step_bias,
    decay_log,
    skip_gain,
    taps_inner,
    taps_input,
    taps_output,
    recent_inner,
    recent_input,
    recent_output,
    states,
    block_inner,
    block_input,
    block_decay,
    lengths,
    norm_gain,
    mixer_out,
    channel_gain,
    expand_gate,
    expand_value,
    reduce_proj,
):
    rows_own = hidden.shape[0]
    seq_all = hidden.shape[1]
    seq_dev = states.shape[0]
    half_dim = states.shape[2]
    width = rows_own * lax.axis_size("kv") * lax.axis_size("tp")
    offset = (lax.axis_index("kv") * lax.axis_size("tp") + lax.axis_index("tp")) * rows_own
    own_start = lax.axis_index("kv") * seq_dev
    whole_rows = lax.all_gather(hidden, ("kv", "tp"), axis=0, tiled=True)
    whole_f = whole_rows.astype(jnp.float32)
    rms_in = lax.rsqrt(jnp.mean(whole_f * whole_f, axis=0) + epsilon)
    normed_in = (whole_f * mixer_gain[:, None]).astype(jnp.bfloat16)
    gate_part = (
        rms_in[:, None, None]
        * jnp.einsum("ds,dhp->shp", normed_in, gate_proj, preferred_element_type=jnp.float32)
    ).astype(jnp.bfloat16)
    inner_part = (
        rms_in[:, None, None]
        * jnp.einsum("ds,dhp->shp", normed_in, inner_proj, preferred_element_type=jnp.float32)
    ).astype(jnp.bfloat16)
    input_part = (
        rms_in[:, None]
        * jnp.einsum("ds,dk->sk", normed_in, input_proj, preferred_element_type=jnp.float32)
    ).astype(jnp.bfloat16)
    output_part = (
        rms_in[:, None]
        * jnp.einsum("ds,dk->sk", normed_in, output_proj, preferred_element_type=jnp.float32)
    ).astype(jnp.bfloat16)
    own_cols = lax.dynamic_slice_in_dim(normed_in, own_start, seq_dev, 1)
    own_rms = lax.dynamic_slice_in_dim(rms_in, own_start, seq_dev, 0)
    step_pre = (
        own_rms[:, None]
        * jnp.einsum("ds,dh->sh", own_cols, step_proj, preferred_element_type=jnp.float32)
    ).astype(jnp.bfloat16)
    gate_pre, inner_pre, input_pre, output_pre = (
        lax.all_to_all(gate_part, "kv", split_axis=0, concat_axis=1, tiled=True),
        lax.all_to_all(inner_part, "kv", split_axis=0, concat_axis=1, tiled=True),
        lax.all_to_all(input_part, "kv", split_axis=0, concat_axis=1, tiled=True),
        lax.all_to_all(output_part, "kv", split_axis=0, concat_axis=1, tiled=True),
    )
    conv_inner = short_conv(recent_inner, inner_pre, taps_inner)
    conv_input = short_conv(recent_input, input_pre, taps_input)
    conv_output = short_conv(recent_output, output_pre, taps_output).astype(jnp.bfloat16)
    step = jax.nn.softplus(step_pre.astype(jnp.float32) + step_bias[None, :])
    new_decay = -jnp.exp(decay_log)[None, :] * step
    per_group = MIXER_HEADS // GROUPS
    live = (jnp.arange(OPEN_BLOCK_SPAN, dtype=jnp.int32)[None, :] < lengths[:, None]).astype(
        jnp.float32
    )
    masked = block_decay * live[:, :, None]
    cached = jnp.sum(masked, axis=1)
    tail = new_decay[:, None, :] + cached[:, None, :] - jnp.cumsum(masked, axis=1)
    total = new_decay + cached
    readout = conv_output.reshape(seq_dev, GROUPS, STATE)
    score = jnp.einsum(
        "sgn,sjgn->sgj",
        readout,
        block_input.reshape(seq_dev, OPEN_BLOCK_SPAN, GROUPS, STATE),
        preferred_element_type=jnp.float32,
    )
    score_heads = jnp.repeat(score, per_group, axis=1)
    weight = (live[:, None, :] * jnp.exp(jnp.swapaxes(tail, 1, 2)) * score_heads).astype(
        jnp.bfloat16
    )
    from_block = jnp.einsum(
        "shj,sjhp->shp", weight, block_inner, preferred_element_type=jnp.float32
    )
    readout_f = readout.astype(jnp.float32)
    grouped = states.reshape(seq_dev, GROUPS, per_group, half_dim, STATE)
    from_state = jnp.einsum(
        "sgn,sgrpn->sgrp", readout_f, grouped, precision=lax.Precision.HIGHEST
    ).reshape(seq_dev, MIXER_HEADS, half_dim)
    own_score = jnp.repeat(
        jnp.sum(readout_f * conv_input.reshape(seq_dev, GROUPS, STATE), axis=-1), per_group, axis=1
    )
    mix = (
        from_block
        + jnp.exp(total)[:, :, None] * from_state
        + (own_score * step)[:, :, None] * conv_inner
        + skip_gain[None, :, None] * conv_inner
    )
    gated_raw = mix * jax.nn.silu(gate_pre.astype(jnp.float32))
    part_squares = jnp.sum(gated_raw * gated_raw, axis=(1, 2))
    gated = (gated_raw * norm_gain[None]).astype(jnp.bfloat16)
    placed = lax.dynamic_update_slice_in_dim(
        jnp.zeros((seq_all,), jnp.float32), part_squares, own_start, 0
    )
    gate_squares = lax.psum(placed, ("kv", "tp"))
    rms_gate = lax.rsqrt(gate_squares / (MIXER_HEADS * HEAD_DIM) + epsilon)
    by_head = lax.all_to_all(gated, "kv", split_axis=1, concat_axis=0, tiled=True)
    columns = mixer_out
    mixed_full = rms_gate[None, :] * lax.psum(
        jnp.einsum("hpd,shp->ds", columns, by_head, preferred_element_type=jnp.float32),
        ("kv", "tp"),
    )
    mid_full = (whole_f + mixed_full).astype(jnp.bfloat16)
    mid = lax.dynamic_slice_in_dim(mid_full, offset, rows_own, 0)
    full_f = mid_full.astype(jnp.float32)
    mid_squares = jnp.sum(full_f * full_f, axis=0)
    normed_full = (full_f * channel_gain[:, None]).astype(jnp.bfloat16)
    gate_sum = jnp.einsum("ds,df->sf", normed_full, expand_gate, preferred_element_type=jnp.float32)
    value_sum = jnp.einsum(
        "ds,df->sf", normed_full, expand_value, preferred_element_type=jnp.float32
    )
    rms_mid = lax.rsqrt(mid_squares / width + epsilon)
    act = (jax.nn.silu(rms_mid[:, None] * gate_sum) * (rms_mid[:, None] * value_sum)).astype(
        jnp.bfloat16
    )
    columns = reduce_proj
    channel = lax.psum_scatter(
        jnp.einsum("fd,sf->ds", columns, act, preferred_element_type=jnp.float32),
        ("kv", "tp"),
        scatter_dimension=0,
        tiled=True,
    )
    return (mid.astype(jnp.float32) + channel).astype(jnp.bfloat16)


NT = (((1,), (1,)), ((), ()))
NN = (((1,), (0,)), ((), ()))
LANES = 128


def dot(a, b, dims, precision=None):
    return lax.dot_general(a, b, dims, precision=precision, preferred_element_type=jnp.float32)


def silu(v):
    return v / (1.0 + jnp.exp(-v))


def tree(values):
    values = list(values)
    while len(values) > 1:
        values = [a + b for a, b in zip(values[::2], values[1::2])]
    return values[0]


def call(body, outs, args, scratch=(), scalars=(), space=pltpu.VMEM):
    args = [pltpu.with_memory_space_constraint(a, pltpu.VMEM) for a in args]
    return pl.pallas_call(
        body,
        out_shape=[space(s, d) for s, d in outs],
        in_specs=[pl.BlockSpec(memory_space=pltpu.VMEM) for _ in args]
        + [pl.BlockSpec(memory_space=pltpu.SMEM) for _ in scalars],
        out_specs=[pl.BlockSpec(memory_space=pltpu.VMEM) for _ in outs],
        scratch_shapes=[pltpu.VMEM(s, d) for s, d in scratch],
        compiler_params=pltpu.CompilerParams(vmem_limit_bytes=8 << 20),
        cost_estimate=pl.CostEstimate(flops=20_000_000_000, bytes_accessed=0, transcendentals=0),
    )(*args, *scalars)


def lane(start, size):
    return pl.ds(pl.multiple_of(start, LANES), size)


def hold(a, out):
    out[...] = a[...]


def stack(a, b, out):
    tp = lax.axis_index("tp")
    part = a.shape[1]
    out[:, lane(tp * part, part)] = a[...]
    out[:, lane((1 - tp) * part, part)] = b[...]


def pack(taps, recent, gain, out):
    n, last = taps.shape[0], out.shape[0] - 1
    out[:n] = taps[...]
    out[n:last] = recent[...].astype(jnp.float32)
    out[last] = gain[...]


def products(piece, base, gain, gate_w, inner_w, input_w, output_w, step_w):
    at = lane(base, piece.shape[1])
    normed = (piece[...].astype(jnp.float32) * gain[:, at]).astype(jnp.bfloat16)
    return (
        dot(normed, gate_w[:, at], NT),
        dot(normed, inner_w[:, at], NT),
        dot(normed, input_w[at, :], NN),
        dot(normed, output_w[at, :], NN),
        dot(normed, step_w[:, at], NT),
    )


def project_own(piece, *refs):
    base = lax.axis_index("kv") * piece.shape[1]
    for out, value in zip(refs[6:], products(piece, base, *refs[:6])):
        out[...] = value


def project(n, *refs):
    pieces, weights, sums = refs[:n], refs[n : n + 6], refs[n + 6 : n + 11]
    x_out, step_out, *sends = refs[n + 11 :]
    kv = lax.axis_index("kv")
    width = x_out.shape[1]
    part = pieces[0].shape[1]
    totals = [ref[...] for ref in sums]
    for k, ref in enumerate(pieces):
        base = (kv ^ k) * part
        x_out[:, lane(base, part)] = ref[...]
        if k:
            totals = [a + b for a, b in zip(totals, products(ref, base, *weights))]
    x = x_out[...].astype(jnp.float32)
    rms = lax.rsqrt(jnp.sum(x * x, axis=1, keepdims=True) / width + epsilon)
    at = 0
    for value in totals[:-1]:
        value = (rms * value).astype(jnp.bfloat16).astype(jnp.float32)
        row = lax.broadcasted_iota(jnp.int32, value.shape, 0)
        for k, ref in enumerate(sends):
            picked = jnp.sum(jnp.where(row == (kv ^ k), value, 0.0), axis=0, keepdims=True)
            ref[:, at : at + value.shape[1]] = picked
        at += value.shape[1]
    steps = (rms * totals[-1]).astype(jnp.bfloat16).astype(jnp.float32)
    row = lax.broadcasted_iota(jnp.int32, steps.shape, 0)
    step_out[...] = jnp.sum(jnp.where(row == kv, steps, 0.0), axis=0, keepdims=True)


def mixer(n, *refs):
    pieces, refs = refs[:n], refs[n:]
    step_pre, step_bias, decay_log, skip_gain = refs[:4]
    packed, taps_input, taps_output, recent_input, recent_output = refs[4:9]
    states, block_inner, block_input, block_decay, length = refs[9:14]
    sends, (gate_row, inner_row, input_row, output_row, gated_row) = refs[14:-5], refs[-5:]
    kv = lax.axis_index("kv")
    heads, span = block_decay.shape
    channels = gate_row.shape[1]
    half = channels // heads
    size = states.shape[1]
    groups = block_input.shape[1] // size
    per_group = heads // groups
    chunk = per_group * half
    cols, maps = channels // n, input_row.shape[1] // n
    for k, ref in enumerate(pieces):
        src = kv ^ k
        gate_row[:, lane(src * cols, cols)] = ref[:, :cols]
        inner_row[:, lane(src * cols, cols)] = ref[:, cols : 2 * cols]
        input_row[:, lane(src * maps, maps)] = ref[:, 2 * cols : 2 * cols + maps]
        output_row[:, lane(src * maps, maps)] = ref[:, 2 * cols + maps :]

    def conv(recent, newest, taps):
        past = jnp.sum(recent.astype(jnp.float32) * taps[:-1], axis=0, keepdims=True)
        return silu(past + taps[-1:] * newest)

    count = taps_input.shape[0]
    conv_output = conv(recent_output[...], output_row[...], taps_output[...]).astype(jnp.bfloat16)
    conv_input = conv(recent_input[...], input_row[...], taps_input[...])
    last = packed.shape[0] - 1
    conv_inner = conv(packed[count:last], inner_row[...], packed[:count])
    norm_gain = packed[last:]
    readout = conv_output.astype(jnp.float32)

    eye = lax.broadcasted_iota(jnp.int32, (heads, heads), 0) == lax.broadcasted_iota(
        jnp.int32, (heads, heads), 1
    )

    def column(row):
        return jnp.sum(jnp.where(eye, row, 0.0), axis=1, keepdims=True)

    pre = step_pre[...] + step_bias[...]
    step_row = jnp.maximum(pre, 0.0) + jnp.log1p(jnp.exp(-jnp.abs(pre)))
    step = column(step_row)
    new_decay = column(-jnp.exp(decay_log[...]) * step_row)
    skip = column(skip_gain[...])

    live = (lax.broadcasted_iota(jnp.int32, (1, span), 1) < length[0]).astype(jnp.float32)
    masked = block_decay[...] * live
    later = (
        lax.broadcasted_iota(jnp.int32, (span, span), 0)
        > lax.broadcasted_iota(jnp.int32, (span, span), 1)
    ).astype(jnp.float32)
    suffix = dot(masked, later, NN, lax.Precision.HIGHEST)
    grown = jnp.exp(new_decay + jnp.sum(masked, axis=1, keepdims=True))
    decayed = live * jnp.exp(new_decay + suffix)

    wide = (groups, groups * size)
    diagonal = lax.broadcasted_iota(jnp.int32, wide, 1) // size == lax.broadcasted_iota(
        jnp.int32, wide, 0
    )
    spread = jnp.where(diagonal, readout, 0.0)
    score = dot(spread.astype(jnp.bfloat16), block_input[...], NT)
    own_score = jnp.sum(spread * conv_input, axis=1, keepdims=True)

    narrow = (per_group, chunk)
    mine = lax.broadcasted_iota(jnp.int32, narrow, 1) // half == lax.broadcasted_iota(
        jnp.int32, narrow, 0
    )
    squares = jnp.zeros((1, chunk), jnp.float32)
    for g in range(groups):
        head = slice(g * per_group, (g + 1) * per_group)
        rows = slice(g * chunk, (g + 1) * chunk)
        weight = decayed[head] * score[g : g + 1]
        out_map = jnp.broadcast_to(readout[:, g * size : (g + 1) * size], (per_group, size))
        left = jnp.concatenate(
            [
                jnp.concatenate([weight, jnp.zeros((per_group, size), jnp.float32)], axis=1),
                jnp.concatenate([jnp.zeros((per_group, span), jnp.float32), out_map], axis=1),
            ],
            axis=0,
        )
        right = jnp.concatenate([block_inner[rows, :], states[rows, :].astype(jnp.bfloat16)], axis=1)
        product = dot(left.astype(jnp.bfloat16), right, NT)
        from_block, from_state = product[:per_group], product[per_group:]
        direct = own_score[g : g + 1] * step[head] + skip[head]
        both = from_block + grown[head] * from_state + direct * conv_inner[:, rows]
        mix = jnp.sum(jnp.where(mine, both, 0.0), axis=0, keepdims=True)
        raw = mix * silu(gate_row[:, rows])
        squares = squares + raw * raw
        gated_row[:, rows] = (raw * norm_gain[:, rows]).astype(jnp.bfloat16).astype(jnp.float32)
    square = jnp.sum(squares, axis=1, keepdims=True)
    for k, ref in enumerate(sends):
        ref[:, :cols] = gated_row[:, lane((kv ^ k) * cols, cols)]
        ref[:, cols:] = jnp.broadcast_to(square, (1, LANES))


def out_project(n, *refs):
    pieces, (mixer_out, out, rows) = refs[:n], refs[n:]
    kv = lax.axis_index("kv")
    cols, width = mixer_out.shape
    for k, ref in enumerate(pieces):
        rows[pl.ds(kv ^ k, 1), :] = ref[...]
    out[:, :width] = dot(rows[:, :cols].astype(jnp.bfloat16), mixer_out[...], NN)
    out[:, width:] = rows[:, cols:]


def add_pair(a, b, out, squares):
    width = out.shape[1]
    out[...] = (a[:, :width] + b[:, :width]).astype(jnp.bfloat16)
    squares[...] = a[:, width:] + b[:, width:]


def channel_mix(n, channels, *refs):
    pieces, (squares, x, gain, gate_w, value_w, reduce_w) = refs[:n], refs[n : n + 6]
    mid_out, keep, send, moved = refs[n + 6 :]
    kv, tp = lax.axis_index("kv"), lax.axis_index("tp")
    width = x.shape[1]
    part = mid_out.shape[1]
    whole = tree(ref[...].astype(jnp.float32) for ref in pieces)
    rms_gate = lax.rsqrt(squares[:, :1] / channels + epsilon)
    mid = (x[...].astype(jnp.float32) + rms_gate * whole).astype(jnp.bfloat16)
    mid = mid.astype(jnp.float32)
    rms = lax.rsqrt(jnp.sum(mid * mid, axis=1, keepdims=True) / width + epsilon)
    normed = (mid * gain[...]).astype(jnp.bfloat16)
    moved[...] = mid
    mid_out[...] = moved[:, lane((kv * 2 + tp) * part, part)]
    act = silu(rms * dot(normed, gate_w[...], NT)) * (rms * dot(normed, value_w[...], NT))
    moved[...] = dot(act.astype(jnp.bfloat16), reduce_w[...], NN)
    for k in range(n):
        at = slice(k * part, (k + 1) * part)
        side = tp if k == 0 else 1 - tp
        keep[:, at] = moved[:, lane((2 * (kv ^ k) + side) * part, part)]
        send[:, at] = moved[:, lane((2 * (kv ^ k) + 1 - side) * part, part)]


def split_pair(a, b, *outs):
    part = outs[0].shape[1]
    for k, ref in enumerate(outs):
        at = slice(k * part, (k + 1) * part)
        ref[...] = a[:, at] + b[:, at]


def finish(n, *refs):
    pieces, (mid, out) = refs[:n], refs[n:]
    out[...] = (mid[...] + tree(ref[...] for ref in pieces)).astype(jnp.bfloat16)


def across(values, first=1):
    n = len(values)
    got = list(values[:first])
    for k in range(first, n):
        pairs = [(i, i ^ (2 * k + 1)) for i in range(2 * n)]
        got.append(lax.ppermute(values[k], ("kv", "tp"), pairs))
    return got


def beside(value):
    return lax.ppermute(value, "tp", [(0, 1), (1, 0)])


def layer(*args):
    (
        hidden, mixer_gain, gate_proj, inner_proj, input_proj, output_proj, step_proj, step_bias,
        decay_log, skip_gain, taps_inner, taps_input, taps_output, recent_inner, recent_input,
        recent_output, states, block_inner, block_input, block_decay, lengths, norm_gain, mixer_out,
        channel_gain, expand_gate, expand_value, reduce_proj,
    ) = args
    n = lax.axis_size("kv")
    part, seqs = hidden.shape
    width = part * n * 2
    heads, half, size = states.shape[1:]
    channels = heads * half
    cols, maps = channels // n, input_proj.shape[1]
    aligned = all(v % LANES == 0 for v in (part, cols, maps, width, size, block_decay.shape[1]))
    if not (
        n & (n - 1) == 0
        and lax.axis_size("tp") == 2
        and states.shape[0] == 1
        and seqs == n
        and aligned
    ):
        return general(*args)
    f32, bf16 = jnp.float32, jnp.bfloat16
    x = hidden.T
    other = beside(x)
    (x,) = call(hold, [((seqs, part), bf16)], [x])
    (pair,) = call(stack, [((seqs, 2 * part), bf16)], [x, other])
    pieces = across([pair] * n)
    taps = taps_inner.shape[0]
    rows = 2 * taps
    (packed,) = call(
        pack,
        [((rows, half, heads), f32)],
        [taps_inner.transpose(0, 2, 1), recent_inner[0].transpose(0, 2, 1), norm_gain.T],
    )
    packed, states, block_inner = (
        beside(v) for v in (packed, states, block_inner)
    )
    weights = [
        mixer_gain.reshape(1, width),
        gate_proj.transpose(1, 2, 0).reshape(cols, width),
        inner_proj.transpose(1, 2, 0).reshape(cols, width),
        input_proj,
        output_proj,
        step_proj.T,
    ]
    sums = call(
        project_own,
        [((seqs, c), f32) for c in (cols, cols, maps, maps, heads)],
        [pair] + weights,
    )
    whole, step_pre, *sends = call(
        functools.partial(project, n),
        [((seqs, width), bf16), ((1, heads), f32)] + [((1, 2 * cols + 2 * maps), f32)] * n,
        pieces + weights + list(sums),
    )
    pieces = across(sends, first=0)
    sends = call(
        functools.partial(mixer, n),
        [((1, cols + LANES), f32)] * n,
        pieces
        + [
            step_pre,
            step_bias.reshape(1, heads),
            decay_log.reshape(1, heads),
            skip_gain.reshape(1, heads),
            packed.transpose(0, 2, 1).reshape(rows, channels),
            taps_input,
            taps_output,
            recent_input[0],
            recent_output[0],
            states.reshape(channels, size),
            block_inner.transpose(0, 2, 3, 1).reshape(channels, -1),
            block_input[0],
            block_decay[0].T,
        ],
        scalars=[lengths],
        scratch=[((1, channels), f32)] * 2 + [((1, n * maps), f32)] * 2 + [((1, channels), f32)],
    )
    pieces = across(sends, first=0)
    (mixed,) = call(
        functools.partial(out_project, n),
        [((seqs, width + LANES), f32)],
        pieces + [mixer_out.reshape(cols, width)],
        scratch=[((seqs, cols + LANES), f32)],
    )
    mixed, squares = call(
        add_pair,
        [((seqs, width), bf16), ((seqs, LANES), f32)],
        [mixed, beside(mixed)],
    )
    pieces = across([mixed] * n)
    mid, keep, send = call(
        functools.partial(channel_mix, n, 2 * channels),
        [((seqs, part), f32)] + [((seqs, width // 2), f32)] * 2,
        pieces
        + [squares, whole, channel_gain.reshape(1, width), expand_gate.T, expand_value.T, reduce_proj],
        scratch=[((seqs, width), f32)],
    )
    sends = call(split_pair, [((seqs, part), f32)] * n, [keep, beside(send)])
    pieces = across(sends)
    (out,) = call(
        functools.partial(finish, n),
        [((seqs, part), bf16)],
        pieces + [mid],
        space=jax.ShapeDtypeStruct,
    )
    return out.T


def solution(mesh):
    return jax.shard_map(
        layer,
        mesh=mesh,
        in_specs=(
            P(("kv", "tp"), "dp"),
            P(),
            P(None, "kv", "tp"),
            P(None, "kv", "tp"),
            P(None, "kv"),
            P(None, "kv"),
            P(),
            P(),
            P(),
            P(),
            P(None, None, "tp"),
            P(),
            P(),
            P(("dp", "kv"), None, None, "tp"),
            P(("dp", "kv"), None, None),
            P(("dp", "kv"), None, None),
            P(("dp", "kv"), None, "tp", None),
            P(("dp", "kv"), None, None, "tp"),
            P(("dp", "kv"), None, None),
            P(("dp", "kv"), None, None),
            P(("dp", "kv")),
            P(None, "tp"),
            P("kv", "tp", None),
            P(),
            P(None, ("kv", "tp")),
            P(None, ("kv", "tp")),
            P(("kv", "tp"), None),
        ),
        out_specs=P(("kv", "tp"), "dp"),
        check_vma=False,
    )
```

```python
import functools

import jax
import jax.numpy as jnp
from jax import lax
from jax.experimental import pallas as pl
from jax.experimental.pallas import tpu as pltpu
from jax.sharding import PartitionSpec as P


MIXER_HEADS = 64
HEAD_DIM = 64
GROUPS = 8
STATE = 128
OPEN_BLOCK_SPAN = 128


epsilon = 1e-05


def short_conv(recent, newest, taps):
    window = jnp.concatenate(
        [recent.astype(jnp.float32), newest.astype(jnp.float32)[:, None]], axis=1
    )
    return jax.nn.silu(jnp.sum(window * taps[None], axis=1))


def general(
    hidden,
    mixer_gain,
    gate_proj,
    inner_proj,
    input_proj,
    output_proj,
    step_proj,
    step_bias,
    decay_log,
    skip_gain,
    taps_inner,
    taps_input,
    taps_output,
    recent_inner,
    recent_input,
    recent_output,
    states,
    block_inner,
    block_input,
    block_decay,
    lengths,
    norm_gain,
    mixer_out,
    channel_gain,
    expand_gate,
    expand_value,
    reduce_proj,
):
    rows_own = hidden.shape[0]
    seq_all = hidden.shape[1]
    seq_dev = states.shape[0]
    half_dim = states.shape[2]
    width = rows_own * lax.axis_size("kv") * lax.axis_size("tp")
    offset = (lax.axis_index("kv") * lax.axis_size("tp") + lax.axis_index("tp")) * rows_own
    own_start = lax.axis_index("kv") * seq_dev
    whole_rows = lax.all_gather(hidden, ("kv", "tp"), axis=0, tiled=True)
    whole_f = whole_rows.astype(jnp.float32)
    rms_in = lax.rsqrt(jnp.mean(whole_f * whole_f, axis=0) + epsilon)
    normed_in = (whole_f * mixer_gain[:, None]).astype(jnp.bfloat16)
    gate_part = (
        rms_in[:, None, None]
        * jnp.einsum("ds,dhp->shp", normed_in, gate_proj, preferred_element_type=jnp.float32)
    ).astype(jnp.bfloat16)
    inner_part = (
        rms_in[:, None, None]
        * jnp.einsum("ds,dhp->shp", normed_in, inner_proj, preferred_element_type=jnp.float32)
    ).astype(jnp.bfloat16)
    input_part = (
        rms_in[:, None]
        * jnp.einsum("ds,dk->sk", normed_in, input_proj, preferred_element_type=jnp.float32)
    ).astype(jnp.bfloat16)
    output_part = (
        rms_in[:, None]
        * jnp.einsum("ds,dk->sk", normed_in, output_proj, preferred_element_type=jnp.float32)
    ).astype(jnp.bfloat16)
    own_cols = lax.dynamic_slice_in_dim(normed_in, own_start, seq_dev, 1)
    own_rms = lax.dynamic_slice_in_dim(rms_in, own_start, seq_dev, 0)
    step_pre = (
        own_rms[:, None]
        * jnp.einsum("ds,dh->sh", own_cols, step_proj, preferred_element_type=jnp.float32)
    ).astype(jnp.bfloat16)
    gate_pre, inner_pre, input_pre, output_pre = (
        lax.all_to_all(gate_part, "kv", split_axis=0, concat_axis=1, tiled=True),
        lax.all_to_all(inner_part, "kv", split_axis=0, concat_axis=1, tiled=True),
        lax.all_to_all(input_part, "kv", split_axis=0, concat_axis=1, tiled=True),
        lax.all_to_all(output_part, "kv", split_axis=0, concat_axis=1, tiled=True),
    )
    conv_inner = short_conv(recent_inner, inner_pre, taps_inner)
    conv_input = short_conv(recent_input, input_pre, taps_input)
    conv_output = short_conv(recent_output, output_pre, taps_output).astype(jnp.bfloat16)
    step = jax.nn.softplus(step_pre.astype(jnp.float32) + step_bias[None, :])
    new_decay = -jnp.exp(decay_log)[None, :] * step
    per_group = MIXER_HEADS // GROUPS
    live = (jnp.arange(OPEN_BLOCK_SPAN, dtype=jnp.int32)[None, :] < lengths[:, None]).astype(
        jnp.float32
    )
    masked = block_decay * live[:, :, None]
    cached = jnp.sum(masked, axis=1)
    tail = new_decay[:, None, :] + cached[:, None, :] - jnp.cumsum(masked, axis=1)
    total = new_decay + cached
    readout = conv_output.reshape(seq_dev, GROUPS, STATE)
    score = jnp.einsum(
        "sgn,sjgn->sgj",
        readout,
        block_input.reshape(seq_dev, OPEN_BLOCK_SPAN, GROUPS, STATE),
        preferred_element_type=jnp.float32,
    )
    score_heads = jnp.repeat(score, per_group, axis=1)
    weight = (live[:, None, :] * jnp.exp(jnp.swapaxes(tail, 1, 2)) * score_heads).astype(
        jnp.bfloat16
    )
    from_block = jnp.einsum(
        "shj,sjhp->shp", weight, block_inner, preferred_element_type=jnp.float32
    )
    readout_f = readout.astype(jnp.float32)
    grouped = states.reshape(seq_dev, GROUPS, per_group, half_dim, STATE)
    from_state = jnp.einsum(
        "sgn,sgrpn->sgrp", readout_f, grouped, precision=lax.Precision.HIGHEST
    ).reshape(seq_dev, MIXER_HEADS, half_dim)
    own_score = jnp.repeat(
        jnp.sum(readout_f * conv_input.reshape(seq_dev, GROUPS, STATE), axis=-1), per_group, axis=1
    )
    mix = (
        from_block
        + jnp.exp(total)[:, :, None] * from_state
        + (own_score * step)[:, :, None] * conv_inner
        + skip_gain[None, :, None] * conv_inner
    )
    gated_raw = mix * jax.nn.silu(gate_pre.astype(jnp.float32))
    part_squares = jnp.sum(gated_raw * gated_raw, axis=(1, 2))
    gated = (gated_raw * norm_gain[None]).astype(jnp.bfloat16)
    placed = lax.dynamic_update_slice_in_dim(
        jnp.zeros((seq_all,), jnp.float32), part_squares, own_start, 0
    )
    gate_squares = lax.psum(placed, ("kv", "tp"))
    rms_gate = lax.rsqrt(gate_squares / (MIXER_HEADS * HEAD_DIM) + epsilon)
    by_head = lax.all_to_all(gated, "kv", split_axis=1, concat_axis=0, tiled=True)
    columns = mixer_out
    mixed_full = rms_gate[None, :] * lax.psum(
        jnp.einsum("hpd,shp->ds", columns, by_head, preferred_element_type=jnp.float32),
        ("kv", "tp"),
    )
    mid_full = (whole_f + mixed_full).astype(jnp.bfloat16)
    mid = lax.dynamic_slice_in_dim(mid_full, offset, rows_own, 0)
    full_f = mid_full.astype(jnp.float32)
    mid_squares = jnp.sum(full_f * full_f, axis=0)
    normed_full = (full_f * channel_gain[:, None]).astype(jnp.bfloat16)
    gate_sum = jnp.einsum("ds,df->sf", normed_full, expand_gate, preferred_element_type=jnp.float32)
    value_sum = jnp.einsum(
        "ds,df->sf", normed_full, expand_value, preferred_element_type=jnp.float32
    )
    rms_mid = lax.rsqrt(mid_squares / width + epsilon)
    act = (jax.nn.silu(rms_mid[:, None] * gate_sum) * (rms_mid[:, None] * value_sum)).astype(
        jnp.bfloat16
    )
    columns = reduce_proj
    channel = lax.psum_scatter(
        jnp.einsum("fd,sf->ds", columns, act, preferred_element_type=jnp.float32),
        ("kv", "tp"),
        scatter_dimension=0,
        tiled=True,
    )
    return (mid.astype(jnp.float32) + channel).astype(jnp.bfloat16)


NT = (((1,), (1,)), ((), ()))
NN = (((1,), (0,)), ((), ()))
LANES = 128


def dot(a, b, dims, precision=None):
    return lax.dot_general(a, b, dims, precision=precision, preferred_element_type=jnp.float32)


def silu(v):
    return v / (1.0 + jnp.exp(-v))


def tree(values):
    values = list(values)
    while len(values) > 1:
        values = [a + b for a, b in zip(values[::2], values[1::2])]
    return values[0]


def call(body, outs, args, scratch=(), scalars=(), space=pltpu.VMEM, flops=20_000_000_000):
    args = [pltpu.with_memory_space_constraint(a, pltpu.VMEM) for a in args]
    return pl.pallas_call(
        body,
        out_shape=[space(s, d) for s, d in outs],
        in_specs=[pl.BlockSpec(memory_space=pltpu.VMEM) for _ in args]
        + [pl.BlockSpec(memory_space=pltpu.SMEM) for _ in scalars],
        out_specs=[pl.BlockSpec(memory_space=pltpu.VMEM) for _ in outs],
        scratch_shapes=[pltpu.VMEM(s, d) for s, d in scratch],
        compiler_params=pltpu.CompilerParams(vmem_limit_bytes=8 << 20),
        cost_estimate=pl.CostEstimate(flops=flops, bytes_accessed=0, transcendentals=0),
    )(*args, *scalars)


def lane(start, size):
    return pl.ds(pl.multiple_of(start, LANES), size)


def hold(a, out):
    out[...] = a[...]


def stack(a, b, out):
    tp = lax.axis_index("tp")
    part = a.shape[1]
    out[:, lane(tp * part, part)] = a[...]
    out[:, lane((1 - tp) * part, part)] = b[...]


def pack(taps, recent, gain, out):
    n, last = taps.shape[0], out.shape[0] - 1
    out[:n] = taps[...]
    out[n:last] = recent[...].astype(jnp.float32)
    out[last] = gain[...]


def products(piece, base, gain, gate_w, inner_w, input_w, output_w, step_w):
    at = lane(base, piece.shape[1])
    normed = (piece[...].astype(jnp.float32) * gain[:, at]).astype(jnp.bfloat16)
    return (
        dot(normed, gate_w[:, at], NT),
        dot(normed, inner_w[:, at], NT),
        dot(normed, input_w[at, :], NN),
        dot(normed, output_w[at, :], NN),
        dot(normed, step_w[:, at], NT),
    )


def project_own(piece, *refs):
    base = lax.axis_index("kv") * piece.shape[1]
    for out, value in zip(refs[6:], products(piece, base, *refs[:6])):
        out[...] = value


def project(n, *refs):
    pieces, weights, sums = refs[:n], refs[n : n + 6], refs[n + 6 : n + 11]
    x_out, step_out, *sends = refs[n + 11 :]
    kv = lax.axis_index("kv")
    width = x_out.shape[1]
    part = pieces[0].shape[1]
    totals = [ref[...] for ref in sums]
    for k, ref in enumerate(pieces):
        base = (kv ^ k) * part
        x_out[:, lane(base, part)] = ref[...]
        if k:
            totals = [a + b for a, b in zip(totals, products(ref, base, *weights))]
    x = x_out[...].astype(jnp.float32)
    rms = lax.rsqrt(jnp.sum(x * x, axis=1, keepdims=True) / width + epsilon)
    at = 0
    for value in totals[:-1]:
        value = (rms * value).astype(jnp.bfloat16).astype(jnp.float32)
        row = lax.broadcasted_iota(jnp.int32, value.shape, 0)
        for k, ref in enumerate(sends):
            picked = jnp.sum(jnp.where(row == (kv ^ k), value, 0.0), axis=0, keepdims=True)
            ref[:, at : at + value.shape[1]] = picked
        at += value.shape[1]
    steps = (rms * totals[-1]).astype(jnp.bfloat16).astype(jnp.float32)
    row = lax.broadcasted_iota(jnp.int32, steps.shape, 0)
    step_out[...] = jnp.sum(jnp.where(row == kv, steps, 0.0), axis=0, keepdims=True)


def flip(a, *refs):
    refs[-1][...] = a[...].T


def mixer(n, *refs):
    pieces, refs = refs[:n], refs[n:]
    step_pre, step_bias, decay_log, skip_gain = refs[:4]
    packed, taps_input, taps_output, recent_input, recent_output = refs[4:9]
    states, block_inner, block_input, block_decay, length = refs[9:14]
    sends, (gate_row, inner_row, input_row, output_row, gated_row) = refs[14:-5], refs[-5:]
    kv = lax.axis_index("kv")
    heads, span = block_decay.shape
    channels = gate_row.shape[1]
    half = channels // heads
    size = states.shape[1]
    groups = block_input.shape[1] // size
    per_group = heads // groups
    chunk = per_group * half
    cols, maps = channels // n, input_row.shape[1] // n
    for k, ref in enumerate(pieces):
        src = kv ^ k
        gate_row[:, lane(src * cols, cols)] = ref[:, :cols]
        inner_row[:, lane(src * cols, cols)] = ref[:, cols : 2 * cols]
        input_row[:, lane(src * maps, maps)] = ref[:, 2 * cols : 2 * cols + maps]
        output_row[:, lane(src * maps, maps)] = ref[:, 2 * cols + maps :]

    def conv(recent, newest, taps):
        past = jnp.sum(recent.astype(jnp.float32) * taps[:-1], axis=0, keepdims=True)
        return silu(past + taps[-1:] * newest)

    count = taps_input.shape[0]
    conv_output = conv(recent_output[...], output_row[...], taps_output[...]).astype(jnp.bfloat16)
    conv_input = conv(recent_input[...], input_row[...], taps_input[...])
    last = packed.shape[0] - 1
    conv_inner = conv(packed[count:last], inner_row[...], packed[:count])
    norm_gain = packed[last:]
    readout = conv_output.astype(jnp.float32)

    eye = lax.broadcasted_iota(jnp.int32, (heads, heads), 0) == lax.broadcasted_iota(
        jnp.int32, (heads, heads), 1
    )

    def column(row):
        return jnp.sum(jnp.where(eye, row, 0.0), axis=1, keepdims=True)

    pre = step_pre[...] + step_bias[...]
    step_row = jnp.maximum(pre, 0.0) + jnp.log1p(jnp.exp(-jnp.abs(pre)))
    step = column(step_row)
    new_decay = column(-jnp.exp(decay_log[...]) * step_row)
    skip = column(skip_gain[...])

    live = (lax.broadcasted_iota(jnp.int32, (1, span), 1) < length[0]).astype(jnp.float32)
    masked = block_decay[...] * live
    later = (
        lax.broadcasted_iota(jnp.int32, (span, span), 0)
        > lax.broadcasted_iota(jnp.int32, (span, span), 1)
    ).astype(jnp.float32)
    suffix = dot(masked, later, NN, lax.Precision.HIGHEST)
    grown = jnp.exp(new_decay + jnp.sum(masked, axis=1, keepdims=True))
    decayed = live * jnp.exp(new_decay + suffix)

    wide = (groups, groups * size)
    diagonal = lax.broadcasted_iota(jnp.int32, wide, 1) // size == lax.broadcasted_iota(
        jnp.int32, wide, 0
    )
    spread = jnp.where(diagonal, readout, 0.0)
    score = dot(spread.astype(jnp.bfloat16), block_input[...], NT)
    own_score = jnp.sum(spread * conv_input, axis=1, keepdims=True)

    narrow = (per_group, chunk)
    mine = lax.broadcasted_iota(jnp.int32, narrow, 1) // half == lax.broadcasted_iota(
        jnp.int32, narrow, 0
    )
    squares = jnp.zeros((1, chunk), jnp.float32)
    for g in range(groups):
        head = slice(g * per_group, (g + 1) * per_group)
        rows = slice(g * chunk, (g + 1) * chunk)
        weight = decayed[head] * score[g : g + 1]
        out_map = jnp.broadcast_to(readout[:, g * size : (g + 1) * size], (per_group, size))
        left = jnp.concatenate(
            [
                jnp.concatenate([weight, jnp.zeros((per_group, size), jnp.float32)], axis=1),
                jnp.concatenate([jnp.zeros((per_group, span), jnp.float32), out_map], axis=1),
            ],
            axis=0,
        )
        right = jnp.concatenate([block_inner[rows, :], states[rows, :].astype(jnp.bfloat16)], axis=1)
        product = dot(left.astype(jnp.bfloat16), right, NT)
        from_block, from_state = product[:per_group], product[per_group:]
        direct = own_score[g : g + 1] * step[head] + skip[head]
        both = from_block + grown[head] * from_state + direct * conv_inner[:, rows]
        mix = jnp.sum(jnp.where(mine, both, 0.0), axis=0, keepdims=True)
        raw = mix * silu(gate_row[:, rows])
        squares = squares + raw * raw
        gated_row[:, rows] = (raw * norm_gain[:, rows]).astype(jnp.bfloat16).astype(jnp.float32)
    square = jnp.sum(squares, axis=1, keepdims=True)
    for k, ref in enumerate(sends):
        ref[:, :cols] = gated_row[:, lane((kv ^ k) * cols, cols)]
        ref[:, cols:] = jnp.broadcast_to(square, (1, LANES))


def out_project(n, *refs):
    pieces, (mixer_out, out, rows) = refs[:n], refs[n:]
    kv = lax.axis_index("kv")
    cols, width = mixer_out.shape
    for k, ref in enumerate(pieces):
        rows[pl.ds(kv ^ k, 1), :] = ref[...]
    out[:, :width] = dot(rows[:, :cols].astype(jnp.bfloat16), mixer_out[...], NN)
    out[:, width:] = rows[:, cols:]


def add_pair(a, b, out, squares):
    width = out.shape[1]
    out[...] = (a[:, :width] + b[:, :width]).astype(jnp.bfloat16)
    squares[...] = a[:, width:] + b[:, width:]


def down(n, act, reduce_w, out, other):
    kv, tp = lax.axis_index("kv"), lax.axis_index("tp")
    part = out.shape[1] // n
    for k in range(n):
        side = tp if (k == 0) != other else 1 - tp
        block = reduce_w[:, lane((2 * (kv ^ k) + side) * part, part)]
        out[:, k * part : (k + 1) * part] = dot(act, block, NN)


def channel_mix(n, channels, *refs):
    pieces, (squares, x, gain, gate_w, value_w, reduce_w) = refs[:n], refs[n : n + 6]
    mid_out, act_out, send, moved = refs[n + 6 :]
    kv, tp = lax.axis_index("kv"), lax.axis_index("tp")
    width = x.shape[1]
    part = mid_out.shape[1]
    whole = tree(ref[...].astype(jnp.float32) for ref in pieces)
    rms_gate = lax.rsqrt(squares[:, :1] / channels + epsilon)
    mid = (x[...].astype(jnp.float32) + rms_gate * whole).astype(jnp.bfloat16)
    mid = mid.astype(jnp.float32)
    rms = lax.rsqrt(jnp.sum(mid * mid, axis=1, keepdims=True) / width + epsilon)
    normed = (mid * gain[...]).astype(jnp.bfloat16)
    moved[...] = mid
    mid_out[...] = moved[:, lane((kv * 2 + tp) * part, part)]
    act = silu(rms * dot(normed, gate_w[...], NN)) * (rms * dot(normed, value_w[...], NN))
    act = act.astype(jnp.bfloat16)
    act_out[...] = act
    down(n, act, reduce_w, send, True)


def keep_own(n, act, reduce_w, out):
    down(n, act[...], reduce_w, out, False)


def split_pair(a, b, *outs):
    part = outs[0].shape[1]
    for k, ref in enumerate(outs):
        at = slice(k * part, (k + 1) * part)
        ref[...] = a[:, at] + b[:, at]


def finish(n, *refs):
    pieces, (mid, out) = refs[:n], refs[n:]
    out[...] = (mid[...] + tree(ref[...] for ref in pieces)).astype(jnp.bfloat16)


def across(values, first=1):
    n = len(values)
    got = list(values[:first])
    for k in range(first, n):
        pairs = [(i, i ^ (2 * k + 1)) for i in range(2 * n)]
        got.append(lax.ppermute(values[k], ("kv", "tp"), pairs))
    return got


def beside(value):
    return lax.ppermute(value, "tp", [(0, 1), (1, 0)])


def layer(*args):
    (
        hidden, mixer_gain, gate_proj, inner_proj, input_proj, output_proj, step_proj, step_bias,
        decay_log, skip_gain, taps_inner, taps_input, taps_output, recent_inner, recent_input,
        recent_output, states, block_inner, block_input, block_decay, lengths, norm_gain, mixer_out,
        channel_gain, expand_gate, expand_value, reduce_proj,
    ) = args
    n = lax.axis_size("kv")
    part, seqs = hidden.shape
    width = part * n * 2
    heads, half, size = states.shape[1:]
    channels = heads * half
    cols, maps = channels // n, input_proj.shape[1]
    aligned = all(v % LANES == 0 for v in (part, cols, maps, width, size, block_decay.shape[1]))
    if not (
        n & (n - 1) == 0
        and lax.axis_size("tp") == 2
        and states.shape[0] == 1
        and seqs == n
        and aligned
    ):
        return general(*args)
    f32, bf16 = jnp.float32, jnp.bfloat16
    x = hidden.T
    other = beside(x)
    (x,) = call(hold, [((seqs, part), bf16)], [x])
    (pair,) = call(stack, [((seqs, 2 * part), bf16)], [x, other])
    pieces = across([pair] * n)
    taps = taps_inner.shape[0]
    rows = 2 * taps
    (packed,) = call(
        pack,
        [((rows, half, heads), f32)],
        [taps_inner.transpose(0, 2, 1), recent_inner[0].transpose(0, 2, 1), norm_gain.T],
    )
    packed, states, block_inner = (
        beside(v) for v in (packed, states, block_inner)
    )
    weights = [
        mixer_gain.reshape(1, width),
        gate_proj.transpose(1, 2, 0).reshape(cols, width),
        inner_proj.transpose(1, 2, 0).reshape(cols, width),
        input_proj,
        output_proj,
        step_proj.T,
    ]
    sums = call(
        project_own,
        [((seqs, c), f32) for c in (cols, cols, maps, maps, heads)],
        [pair] + weights,
    )
    whole, step_pre, *sends = call(
        functools.partial(project, n),
        [((seqs, width), bf16), ((1, heads), f32)] + [((1, 2 * cols + 2 * maps), f32)] * n,
        pieces + weights + list(sums),
    )
    pieces = across(sends, first=0)
    sends = call(
        functools.partial(mixer, n),
        [((1, cols + LANES), f32)] * n,
        pieces
        + [
            step_pre,
            step_bias.reshape(1, heads),
            decay_log.reshape(1, heads),
            skip_gain.reshape(1, heads),
            packed.transpose(0, 2, 1).reshape(rows, channels),
            taps_input,
            taps_output,
            recent_input[0],
            recent_output[0],
            states.reshape(channels, size),
            block_inner.transpose(0, 2, 3, 1).reshape(channels, -1),
            block_input[0],
            block_decay[0].T,
        ],
        scalars=[lengths],
        scratch=[((1, channels), f32)] * 2 + [((1, n * maps), f32)] * 2 + [((1, channels), f32)],
    )
    pieces = across(sends, first=0)
    hidden_units = reduce_proj.shape[0]
    (gate_w,) = call(
        flip,
        [((width, hidden_units), bf16)],
        [expand_gate.T, mixer_out.reshape(cols, width)],
        flops=1,
    )
    (mixed,) = call(
        functools.partial(out_project, n),
        [((seqs, width + LANES), f32)],
        pieces + [mixer_out.reshape(cols, width)],
        scratch=[((seqs, cols + LANES), f32)],
    )
    mixed, squares = call(
        add_pair,
        [((seqs, width), bf16), ((seqs, LANES), f32)],
        [mixed, beside(mixed)],
    )
    pieces = across([mixed] * n)
    (value_w,) = call(flip, [((width, hidden_units), bf16)], [expand_value.T], flops=1)
    mid, act, send = call(
        functools.partial(channel_mix, n, 2 * channels),
        [((seqs, part), f32), ((seqs, hidden_units), bf16), ((seqs, width // 2), f32)],
        pieces
        + [squares, whole, channel_gain.reshape(1, width), gate_w, value_w, reduce_proj],
        scratch=[((seqs, width), f32)],
    )
    other = beside(send)
    (keep,) = call(
        functools.partial(keep_own, n),
        [((seqs, width // 2), f32)],
        [act, reduce_proj],
        flops=1,
    )
    sends = call(split_pair, [((seqs, part), f32)] * n, [keep, other])
    pieces = across(sends)
    (out,) = call(
        functools.partial(finish, n),
        [((seqs, part), bf16)],
        pieces + [mid],
        space=jax.ShapeDtypeStruct,
    )
    return out.T


def solution(mesh):
    return jax.shard_map(
        layer,
        mesh=mesh,
        in_specs=(
            P(("kv", "tp"), "dp"),
            P(),
            P(None, "kv", "tp"),
            P(None, "kv", "tp"),
            P(None, "kv"),
            P(None, "kv"),
            P(),
            P(),
            P(),
            P(),
            P(None, None, "tp"),
            P(),
            P(),
            P(("dp", "kv"), None, None, "tp"),
            P(("dp", "kv"), None, None),
            P(("dp", "kv"), None, None),
            P(("dp", "kv"), None, "tp", None),
            P(("dp", "kv"), None, None, "tp"),
            P(("dp", "kv"), None, None),
            P(("dp", "kv"), None, None),
            P(("dp", "kv")),
            P(None, "tp"),
            P("kv", "tp", None),
            P(),
            P(None, ("kv", "tp")),
            P(None, ("kv", "tp")),
            P(("kv", "tp"), None),
        ),
        out_specs=P(("kv", "tp"), "dp"),
        check_vma=False,
    )
```
